32 devices in a mesh: sp: 16 (over z, y, x), tp: 2 (over core).
Axes of the slice: x: 2, y: 2, z: 4, core: 2. Of those that a mesh axis runs over, the one named last changes fastest.
Arguments:
- stream: bfloat16 [4096, 2048], P(('sp', 'tp')), may hold values from -6 to 6
- queries: bfloat16 [4096, 1024], P('sp', 'tp'), may hold values from -6 to 6
- keys_in: bfloat16 [4096, 1024], P('sp', 'tp'), may hold values from -6 to 6
- values_in: bfloat16 [4096, 1024], P('sp', 'tp'), may hold values from -6 to 6
- gate_in: bfloat16 [4096, 1024], P('sp', 'tp'), may hold values from -6 to 6
- log_decay: float32 [4096, 8], P('sp', 'tp'), may hold values from -0.8 to 0
- head_gain: bfloat16 [1024], P('tp'), may hold values from 0.099609375 to 1.8984375
- out_weight: bfloat16 [1024, 2048], P('tp'), may hold values from -0.1875 to 0.1875
- norm_gain: bfloat16 [2048], replicated, may hold values from 0.099609375 to 1.8984375
- gate_weight: bfloat16 [2048, 5632], P('sp', 'tp'), may hold values from -0.125 to 0.125
- up_weight: bfloat16 [2048, 5632], P('sp', 'tp'), may hold values from -0.125 to 0.125
- down_weight: bfloat16 [5632, 2048], P('tp', 'sp'), may hold values from -0.078125 to 0.078125
Outputs:
- result: bfloat16 [4096, 2048], P(('sp', 'tp'))
The draws below stay inside these ranges and needn't reach their ends.
All inputs are finite; a program needn't handle non-finite values.
Results may differ from the reference program's by a relative error of at most 0.02.
Values may be sent and summed in bfloat16 or wider, within the bound.
A program may use at most 128 MiB of HBM per device.

```python
import jax
import jax.numpy as jnp
from jax import lax

D = 2048
HEAD_COUNT = 8
HEAD_DIM = 128
FF = 5632
BLOCK = 128
TOK_DEV = 256
TOKEN_COUNT = 4096
N_TP = 2


def draw_log_decay(key, part):
    draw_keys = jax.random.split(jax.random.fold_in(key, 11), 7)
    is_fast = jax.random.randint(draw_keys[0], (HEAD_COUNT,), 0, 2) == 0
    slow_rate = jax.random.uniform(draw_keys[1], (HEAD_COUNT,), jnp.float32, 0.2, 0.6) / TOKEN_COUNT
    fast_rate = 1.0 / jax.random.uniform(draw_keys[2], (HEAD_COUNT,), jnp.float32, 30.0, 100.0)
    head_rate = jnp.where(is_fast, fast_rate, slow_rate)
    block_count = TOKEN_COUNT // TOK_DEV
    block_factor = jax.random.uniform(draw_keys[3], (block_count, 1, HEAD_COUNT), jnp.float32, 0.4, 1.6)
    roughness = jax.random.uniform(draw_keys[4], (block_count, TOK_DEV, HEAD_COUNT), jnp.float32, 0.5, 1.5)
    drawn_reference = -(head_rate * block_factor * roughness).reshape(TOKEN_COUNT, HEAD_COUNT)
    spike_locations = jax.random.randint(draw_keys[5], (2, HEAD_COUNT), 0, TOKEN_COUNT)
    spike_drops = jnp.log(jax.random.uniform(draw_keys[6], (2, HEAD_COUNT), jnp.float32, 0.5, 0.8))
    token_positions = jnp.arange(TOKEN_COUNT)[:, None]
    spike_events = jnp.sum(jnp.where(token_positions[None] == spike_locations[:, None, :], spike_drops[:, None, :], 0.0), axis=0)
    return drawn_reference + spike_events


def level_of(own_key, extent, cuts, smallest, largest):
    level = 1.0
    for position, blocks in cuts:
        heights = jax.random.uniform(jax.random.fold_in(jax.random.fold_in(own_key, 6), position), (blocks,), jnp.float32, smallest / len(cuts), largest / len(cuts))
        level = level * jnp.repeat(jnp.exp(heights), extent[position] // blocks).reshape((-1,) + (1,) * (len(extent) - 1 - position))
    return level


def centred(own_key, extent, scale, bound, cuts=(), held_as=jnp.bfloat16):
    drawn = scale * jax.random.normal(own_key, extent, jnp.float32)
    if cuts:
        drawn = drawn * level_of(own_key, extent, cuts, -0.22, 0.18)
    return jnp.clip(drawn, -bound, bound).astype(held_as)


def setup_inputs(seed: int = 0) -> dict:
    streams_of = jax.random.split(jax.random.key(seed), 13)
    return {
        "stream": centred(streams_of[0], (TOKEN_COUNT, D), 0.7, 6.0, ((0, 32),)),
        "queries": centred(streams_of[1], (TOKEN_COUNT, HEAD_COUNT * HEAD_DIM), 1.0, 6.0, ((0, 16), (1, 2))),
        "keys_in": centred(streams_of[2], (TOKEN_COUNT, HEAD_COUNT * HEAD_DIM), 1.0, 6.0, ((0, 16), (1, 2))),
        "values_in": centred(streams_of[3], (TOKEN_COUNT, HEAD_COUNT * HEAD_DIM), 1.0, 6.0, ((0, 16), (1, 2))),
        "gate_in": centred(streams_of[4], (TOKEN_COUNT, HEAD_COUNT * HEAD_DIM), 1.0, 6.0, ((0, 16), (1, 2))),
        "log_decay": draw_log_decay(jax.random.fold_in(streams_of[12], 71), 0),
        "head_gain": jnp.clip(1.0 + 0.18 * jax.random.normal(streams_of[6], (HEAD_COUNT * HEAD_DIM,), jnp.float32), 0.099609375, 1.8984375).astype(jnp.bfloat16),
        "out_weight": centred(streams_of[7], (HEAD_COUNT * HEAD_DIM, D), (HEAD_COUNT * HEAD_DIM) ** -0.5, 0.1875, ((0, 2),)),
        "norm_gain": jnp.clip(1.0 + 0.18 * jax.random.normal(streams_of[8], (D,), jnp.float32), 0.099609375, 1.8984375).astype(jnp.bfloat16),
        "gate_weight": centred(streams_of[9], (D, FF), D ** -0.5, 0.125, ((0, 16), (1, 2))),
        "up_weight": centred(streams_of[10], (D, FF), D ** -0.5, 0.125, ((0, 16), (1, 2))),
        "down_weight": centred(streams_of[11], (FF, D), FF ** -0.5, 0.078125, ((0, 2), (1, 16))),
    }


epsilon = 1e-06
highest = lax.Precision.HIGHEST

def block_pass(state, block_inputs):
    query_block, key_block, value_block, decay_block = block_inputs
    head_dim = query_block.shape[-1]
    key_scale = head_dim ** (-0.5)
    running = jnp.cumsum(decay_block, axis=0)
    query_wide = query_block.astype(jnp.float32)
    key_plain = key_block.astype(jnp.float32)
    value_wide = value_block.astype(jnp.float32)
    scores = jnp.einsum('ihd,jhd->hij', query_wide, key_plain, precision=highest) * key_scale
    offsets = jnp.arange(decay_block.shape[0])
    causal = offsets[:, None] >= offsets[None, :]
    log_gap = running.T[:, :, None] - running.T[:, None, :]
    decay_table = jnp.where(causal[None], jnp.exp(jnp.minimum(log_gap, 0.0)), 0.0)
    within = jnp.einsum('hij,jhe->ihe', scores * decay_table, value_wide, precision=highest)
    carried = jnp.einsum('ihd,hde->ihe', query_wide * jnp.exp(running)[:, :, None], state, precision=highest)
    block_total = running[-1]
    key_wide = key_plain * key_scale * jnp.exp(block_total[None] - running)[:, :, None]
    state = jnp.exp(block_total)[:, None, None] * state + jnp.einsum('jhd,jhe->hde', key_wide, value_wide, precision=highest)
    return (state, within + carried)

def reference(stream, queries, keys_in, values_in, gate_in, log_decay, head_gain, out_weight, norm_gain, gate_weight, up_weight, down_weight):
    heads = log_decay.shape[1]
    head_dim = queries.shape[1] // heads
    block_count = TOKEN_COUNT // BLOCK
    block_shape = (block_count, BLOCK, heads, head_dim)
    block_inputs = (queries.reshape(block_shape), keys_in.reshape(block_shape), values_in.reshape(block_shape), log_decay.reshape(block_count, BLOCK, heads))
    start_state = jnp.zeros((heads, head_dim, head_dim), jnp.float32)
    final_state, retained = lax.scan(block_pass, start_state, block_inputs)
    retained = retained.reshape(TOKEN_COUNT, heads, head_dim)
    center = lax.optimization_barrier(jnp.mean(retained, axis=-1, keepdims=True))
    spread = lax.optimization_barrier(jnp.mean(jnp.square(retained - center), axis=-1, keepdims=True))
    normed_heads = (retained - center) * lax.rsqrt(spread + epsilon) * head_gain.astype(jnp.float32).reshape(heads, head_dim)
    mixed = (jax.nn.silu(gate_in.astype(jnp.float32)) * normed_heads.reshape(TOKEN_COUNT, heads * head_dim)).astype(jnp.bfloat16)
    group_width = heads * head_dim // N_TP
    attended = jnp.zeros((TOKEN_COUNT, D), jnp.float32)
    for group_index in range(N_TP):
        lo_col = group_index * group_width
        group_term = jnp.dot(mixed[:, lo_col:lo_col + group_width], out_weight[lo_col:lo_col + group_width], preferred_element_type=jnp.float32)
        attended = attended + lax.optimization_barrier(group_term.astype(jnp.bfloat16)).astype(jnp.float32)
    residual = stream.astype(jnp.float32) + attended
    normed = (residual * lax.rsqrt(lax.optimization_barrier(jnp.mean(residual * residual, axis=-1, keepdims=True)) + epsilon) * norm_gain.astype(jnp.float32)).astype(jnp.bfloat16)
    gate_sum = jnp.dot(normed, gate_weight, preferred_element_type=jnp.float32)
    up_sum = jnp.dot(normed, up_weight, preferred_element_type=jnp.float32)
    hidden = (jax.nn.silu(gate_sum) * up_sum).astype(jnp.bfloat16)
    unit_width = FF // N_TP
    mixer_out = jnp.zeros((TOKEN_COUNT, D), jnp.float32)
    for group_index in range(N_TP):
        lo_unit = group_index * unit_width
        group_term = jnp.dot(hidden[:, lo_unit:lo_unit + unit_width], down_weight[lo_unit:lo_unit + unit_width], preferred_element_type=jnp.float32)
        mixer_out = mixer_out + lax.optimization_barrier(group_term.astype(jnp.bfloat16)).astype(jnp.float32)
    return (residual + mixer_out).astype(jnp.bfloat16)
```

```python
import functools

import jax
import jax.numpy as jnp
from jax import lax
from jax.experimental import pallas as pl
from jax.experimental.pallas import tpu as pltpu
from jax.sharding import Mesh, PartitionSpec as P

epsilon = 1e-06
GROUP = 4
SP = ("far", "near")
f32, bf16 = jnp.float32, jnp.bfloat16


def swap(value, axis, bits):
    size = lax.axis_size(axis)
    return lax.ppermute(value, axis, [(i, i ^ bits) for i in range(size)])


def near_blocks(value):
    size = lax.axis_size("near")
    steps = (1, 2) if size == 4 else range(1, size)
    return [value] + [swap(value, "near", s) for s in steps]


def near_rest(blocks):
    half = blocks[0].shape[0] // 2
    cut = [(block[:half], block[half:]) for block in blocks]
    if lax.axis_size("near") == 4:
        cut.append((swap(cut[1][0], "near", 2), swap(cut[2][1], "near", 1)))
    return cut


def spread_weights(gate_weight, up_weight, down_weight):
    groups = lax.axis_size("far")
    far_at = lax.axis_index("far")
    width = gate_weight.shape[1] // groups
    all_rows, all_columns = [], []
    for s in range(groups):
        at = (far_at ^ s) * width
        rows = jnp.concatenate(
            [
                lax.dynamic_slice_in_dim(gate_weight, at, width, 1),
                lax.dynamic_slice_in_dim(up_weight, at, width, 1),
            ],
            axis=0,
        )
        all_rows.append(swap(rows, "far", s) if s else rows)
    for s in range(groups):
        at = (far_at ^ s) * width
        all_columns.append(lax.dynamic_slice_in_dim(down_weight, at, width, 0))
    return [near_blocks(piece) for piece in all_rows], all_columns


def by_distance(value):
    groups, near = lax.axis_size("far"), lax.axis_size("near")
    here = lax.axis_index("far") * near + lax.axis_index("near")
    width = value.shape[1] // (groups * near)
    return jnp.concatenate(
        [
            lax.dynamic_slice_in_dim(value, (here ^ k) * width, width, 1)
            for k in range(groups * near)
        ],
        axis=1,
    )


def turned(value, bits):
    groups = lax.axis_size("far")
    width = value.shape[1] // groups
    return jnp.concatenate(
        [value[:, (g ^ bits) * width : ((g ^ bits) + 1) * width] for g in range(groups)], axis=1
    )


def gather_pair(rows):
    if lax.axis_size("tp") == 2:
        return jnp.concatenate([rows, swap(rows, "tp", 1)], axis=0)
    return lax.all_gather(rows, "tp", axis=0, tiled=True)


def scatter_pair(terms):
    terms = terms.astype(bf16)
    if lax.axis_size("tp") == 2:
        half = terms.shape[0] // 2
        return terms[:half].astype(f32) + swap(terms[half:], "tp", 1).astype(f32)
    return lax.psum_scatter(terms, "tp", scatter_dimension=0, tiled=True).astype(f32)


def dot(a, b, dims=((1,), (0,))):
    return lax.dot_general(a, b, (dims, ((), ())), preferred_element_type=f32)


def retention(queries, keys_in, values_in, log_decay):
    row_count, heads = log_decay.shape
    dim = queries.shape[1] // heads
    scale = dim ** (-0.5)
    running = jnp.cumsum(log_decay, axis=0)
    total = running[-1]
    offsets = jnp.arange(row_count)
    causal = offsets[:, None] >= offsets[None, :]
    within, states = [], []
    for h in range(heads):
        cut = slice(h * dim, (h + 1) * dim)
        q, k, v = queries[:, cut], keys_in[:, cut], values_in[:, cut]
        col = running[:, h]
        gap = jnp.minimum(col[:, None] - col[None, :], 0.0)
        table = jnp.where(causal, jnp.exp(gap), 0.0) * scale
        within.append(dot((dot(q, k, ((1,), (1,))) * table).astype(bf16), v))
        tail = (jnp.exp(total[h] - col) * scale)[:, None]
        states.append(dot((k.astype(f32) * tail).astype(bf16), v, ((0,), (0,))))
    return running, total, within, jnp.concatenate(states, axis=0)


def incoming_states(total, state, columns):
    heads = total.shape[0]
    near = lax.axis_size("near")
    here = lax.axis_index("far") * near + lax.axis_index("near")
    high = lax.reduce_precision(total, 8, 7)
    mid = lax.reduce_precision(total - high, 8, 7)
    low = total - high - mid
    parts = jnp.concatenate([high, mid, low])
    extra = -(-parts.shape[0] // 16) * 16
    parts = jnp.pad(parts, (0, extra - parts.shape[0]))
    width = state.shape[1]
    packed = jnp.concatenate(
        [state.astype(bf16), jnp.broadcast_to(parts[:, None], (extra, width)).astype(bf16)], axis=0
    )
    everything = lax.all_gather(packed, SP)
    everything, columns = lax.optimization_barrier((everything, columns))
    columns = [swap(piece, "far", s) if s else piece for s, piece in enumerate(columns)]
    count = everything.shape[0]
    logs = everything[:, state.shape[0] : state.shape[0] + 3 * heads, 0].astype(f32)
    logs = logs.reshape(count, 3, heads).sum(axis=1)
    index = jnp.arange(count)
    between = (index[None, :] > index[:, None]) & (index[None, :] < here)
    reach = jnp.sum(jnp.where(between[:, :, None], logs[None], 0.0), axis=1)
    factor = jnp.where((index < here)[:, None], jnp.exp(reach), 0.0)
    states = everything[:, : state.shape[0]].reshape(count, heads, -1, width)
    return jnp.sum(factor[:, :, None, None] * states.astype(f32), axis=0), columns


def local(
    stream,
    queries,
    keys_in,
    values_in,
    gate_in,
    log_decay,
    head_gain,
    out_weight,
    norm_gain,
    gate_weight,
    up_weight,
    down_weight,
):
    weight_rows, weight_columns = spread_weights(gate_weight, up_weight, down_weight)
    heads = log_decay.shape[1]
    dim = queries.shape[1] // heads
    running, total, within, state = retention(queries, keys_in, values_in, log_decay)
    incoming, weight_columns = incoming_states(total, state, weight_columns)
    mixed = []
    for h in range(heads):
        cut = slice(h * dim, (h + 1) * dim)
        carried = dot(queries[:, cut], incoming[h].astype(bf16))
        retained = within[h] + carried * jnp.exp(running[:, h])[:, None]
        center = jnp.mean(retained, axis=-1, keepdims=True)
        spread = jnp.mean(jnp.square(retained - center), axis=-1, keepdims=True)
        normed = (retained - center) * lax.rsqrt(spread + epsilon) * head_gain[cut].astype(f32)
        mixed.append((jax.nn.silu(gate_in[:, cut].astype(f32)) * normed).astype(bf16))
    terms = dot(jnp.concatenate(mixed, axis=1), out_weight).astype(bf16)
    if lax.axis_size("tp") == 2:
        half = terms.shape[0] // 2
        mine = lax.axis_index("tp") * half
        sent = swap(lax.dynamic_slice_in_dim(terms, half - mine, half, 0), "tp", 1)
        kept = lax.dynamic_slice_in_dim(terms, mine, half, 0)
        attended = kept.astype(f32) + sent.astype(f32)
    else:
        attended = scatter_pair(terms)
    residual = stream.astype(f32) + attended
    normed = (
        residual
        * lax.rsqrt(jnp.mean(residual * residual, axis=-1, keepdims=True) + epsilon)
        * norm_gain.astype(f32)
    ).astype(bf16)

    normed = by_distance(normed)
    normed, weight_rows, weight_columns = lax.optimization_barrier(
        (normed, weight_rows, weight_columns)
    )
    weight_rows = [block for piece in weight_rows for block in near_rest(piece)]
    weight_columns = [
        block for piece in weight_columns for block in near_rest(near_blocks(piece))
    ]
    groups = lax.axis_size("far")
    arrived = [normed] + [swap(normed, "far", s) for s in range(1, groups)]
    rows = [turned(gather_pair(piece), s) for s, piece in enumerate(arrived)]
    gate_full = jnp.concatenate([gate for gate, _ in weight_rows], axis=0)
    up_full = jnp.concatenate([up for _, up in weight_rows], axis=0)
    down_full = jnp.concatenate(
        [jnp.concatenate([part[i] for part in weight_columns], axis=1) for i in range(2)], axis=0
    )
    together = jnp.concatenate(rows, axis=0)
    hidden = (jax.nn.silu(dot(together, gate_full)) * dot(together, up_full)).astype(bf16)
    height = rows[0].shape[0]
    mixer_out = 0.0
    for s in (*range(1, groups), 0):
        part = scatter_pair(dot(hidden[s * height : (s + 1) * height], down_full))
        if s:
            part = turned(swap(part.astype(bf16), "far", s).astype(f32), s)
        mixer_out = mixer_out + part
    return (residual + by_distance(mixer_out)).astype(bf16)


MESH = pl.DeviceIdType.MESH
HIGHEST = lax.Precision.HIGHEST
TAIL = 16


def fits(mesh):
    return mesh.shape["tp"] == 2 and mesh.shape["sp"] == GROUP * GROUP


def flip(v, d):
    if d == 0:
        return v
    if d == 1:
        return v + 1 - 2 * lax.rem(v, 2)
    if d == 2:
        return lax.rem(v + 2, 4)
    return 3 - v


def layer_kernel(
    stream_ref,
    q_ref,
    k_ref,
    v_ref,
    gate_ref,
    decay_ref,
    head_gain_ref,
    out_weight_ref,
    norm_gain_ref,
    wide_ref,
    down_ref,
    result_ref,
    wide,
    down,
    rows,
    residual,
    run_col,
    within,
    state_out,
    state_in,
    plane_out,
    plane_in,
    carry,
    reach,
    entry_out,
    entry_in,
    mixed,
    term_out,
    term_in,
    part_out,
    part_own,
    part_in,
    sum_out,
    sum_in,
    w_send,
    w_relay,
    w_recv,
    w_far,
    st_send,
    st_recv,
    pl_send,
    pl_recv,
    en_send,
    en_recv,
    term_sem,
    row_send,
    row_recv,
    part_sem,
    part_recv,
    sum_send,
    sum_recv,
):
    sp, c = lax.axis_index("sp"), lax.axis_index("tp")
    z, n = lax.div(sp, 4), lax.rem(sp, 4)
    other = 1 - c
    beside = [flip(n, d) for d in range(4)]

    def at(zz, nn, cc):
        return (zz * 4 + nn, cc)

    mate = at(z, n, other)

    def copy(src, dst, send, recv, to):
        return pltpu.make_async_remote_copy(
            src_ref=src,
            dst_ref=dst,
            send_sem=send,
            recv_sem=recv,
            device_id=to,
            device_id_type=MESH,
        )

    def arrived(ref, recv):
        copy(ref, ref, recv, recv, mate).wait_recv()

    def left(ref, send):
        copy(ref, ref, send, send, mate).wait_send()

    barrier = pltpu.get_barrier_semaphore()
    partners = [mate]
    partners += [at(z, beside[d], c) for d in (1, 2, 3)]
    partners += [at(flip(z, d), n, c) for d in (1, 2, 3)]
    for to in partners:
        pl.semaphore_signal(barrier, inc=1, device_id=to, device_id_type=MESH)
    pl.semaphore_wait(barrier, len(partners))

    full = (wide, down)
    given = (wide_ref, down_ref)
    cut = (wide.shape[1] // 2, down.shape[1] // 2)

    def far(d, kind):
        zt = flip(z, d)
        copy(
            given[kind].at[zt],
            full[kind].at[sp],
            w_far.at[kind, d - 1],
            w_recv.at[kind, sp, 0],
            at(zt, n, c),
        ).start()

    def push(d, kind):
        slot = flip(z, d) * 4 + n
        if d:
            arrived(full[kind].at[slot], w_recv.at[kind, slot, 0])
        src = full[kind].at[slot] if d else given[kind].at[z]
        for a in (1, 2):
            copy(
                src,
                full[kind].at[slot],
                w_send.at[kind, d, a - 1],
                w_recv.at[kind, slot, 0],
                at(z, beside[a], c),
            ).start()

    def relay(d, kind):
        half = cut[kind]
        for a in (1, 2):
            slot = flip(z, d) * 4 + beside[a]
            arrived(full[kind].at[slot], w_recv.at[kind, slot, 0])
            part = pl.ds(0, half) if a == 1 else pl.ds(half, half)
            piece = full[kind].at[slot, part]
            copy(
                piece,
                piece,
                w_relay.at[kind, d, a - 1],
                w_recv.at[kind, slot, a - 1],
                at(z, beside[3 - a], c),
            ).start()

    def finish(d, kind):
        half = cut[kind]
        slot = flip(z, d) * 4 + beside[3]
        arrived(full[kind].at[slot, pl.ds(0, half)], w_recv.at[kind, slot, 0])
        arrived(full[kind].at[slot, pl.ds(half, half)], w_recv.at[kind, slot, 1])

    def settle_weights():
        for kind in (0, 1):
            half = cut[kind]
            for d in range(4):
                if d:
                    left(given[kind].at[0], w_far.at[kind, d - 1])
                for a in (0, 1):
                    left(given[kind].at[0], w_send.at[kind, d, a])
                    left(full[kind].at[0, pl.ds(0, half)], w_relay.at[kind, d, a])

    push(0, 1)
    far(1, 1)

    heads = decay_ref.shape[1]
    dim = q_ref.shape[1] // heads
    count = q_ref.shape[0]
    scale = dim ** (-0.5)
    decay = decay_ref[...]
    low = lax.broadcasted_iota(jnp.int32, (count, count), 0)
    high = lax.broadcasted_iota(jnp.int32, (count, count), 1)
    causal = low >= high
    running = jnp.dot(
        causal.astype(f32), decay, precision=HIGHEST, preferred_element_type=f32
    )
    run_col[...] = running
    line = lax.broadcasted_iota(jnp.int32, (TAIL, dim), 0)
    for h in range(heads):
        side = slice(h * dim, (h + 1) * dim)
        col = running[:, h : h + 1]
        total = running[count - 1 : count, h : h + 1]
        tail = jnp.exp(total - col) * scale
        keyed = (k_ref[:, side].astype(f32) * tail).T.astype(bf16)
        state = jnp.dot(keyed, v_ref[:, side], preferred_element_type=f32)
        state_out[h, :dim] = state.astype(bf16)
        state_out[h, dim:] = split_total(total, line)

    for d in (1, 2, 3):
        copy(
            state_out.at[beside[d]],
            state_in.at[n],
            st_send.at[d - 1],
            st_recv.at[d - 1],
            at(z, beside[d], c),
        ).start()
    state_in[n] = state_out[n]
    push(0, 0)
    far(1, 0)

    wide[sp] = wide_ref[z]
    down[sp] = down_ref[z]

    for d in (1, 2, 3):
        arrived(state_in.at[beside[d]], st_recv.at[d - 1])
    totals = [join_total(state_in[m, dim:]) for m in range(4)]
    states = [state_in[m, :dim].astype(f32) for m in range(4)]
    plane, span = states[0], totals[0]
    for m in range(1, 4):
        plane = plane * jnp.exp(totals[m]) + states[m]
        span = span + totals[m]
    plane_out[:dim] = plane.astype(bf16)
    plane_out[dim:] = split_total(span, line)
    for k in (1, 2, 3):

        @pl.when(z + k <= 3)
        def _():
            copy(
                plane_out,
                plane_in.at[z],
                pl_send.at[k - 1],
                pl_recv.at[z],
                at(z + k, n, c),
            ).start()

    far(2, 1)
    far(2, 0)
    far(3, 1)
    far(3, 0)

    for h in range(heads):
        side = slice(h * dim, (h + 1) * dim)
        q, k, v = q_ref[:, side], k_ref[:, side], v_ref[:, side]
        col = jnp.broadcast_to(running[:, h : h + 1], (count, dim))
        row = col.T[0:1]
        gap = jnp.minimum(running[:, h : h + 1] - row, 0.0)
        table = jnp.where(causal, jnp.exp(gap), 0.0) * scale
        scores = dot(q, k, ((1,), (1,)))
        within[:, side] = jnp.dot(
            (scores * table).astype(bf16), v, preferred_element_type=f32
        )

    carry[...] = jnp.zeros_like(carry)
    reach[...] = jnp.zeros_like(reach)
    for k in (1, 2, 3):

        @pl.when(z >= k)
        def _():
            arrived(plane_in.at[z - k], pl_recv.at[z - k])
            carry[...] += jnp.exp(reach[...]) * plane_in[z - k, :dim].astype(f32)
            reach[...] += join_total(plane_in[z - k, dim:])

    entry = carry[...]
    for m in range(4):
        entry_out[m] = entry.astype(bf16)
        if m < 3:
            entry = entry * jnp.exp(totals[m]) + states[m]
    for d in (1, 2, 3):
        copy(
            entry_out.at[beside[d]],
            entry_in.at[n],
            en_send.at[d - 1],
            en_recv.at[d - 1],
            at(z, beside[d], c),
        ).start()
    entry_in[n] = entry_out[n]

    for kind in (1, 0):
        relay(0, kind)
        push(1, kind)

    for d in (1, 2, 3):
        arrived(entry_in.at[beside[d]], en_recv.at[d - 1])
    for h in range(heads):
        side = slice(h * dim, (h + 1) * dim)
        carried = jnp.dot(q_ref[:, side], entry_in[h], preferred_element_type=f32)
        retained = within[:, side] + carried * jnp.exp(run_col[:, h : h + 1])
        center = jnp.mean(retained, axis=-1, keepdims=True)
        away = retained - center
        spread = jnp.mean(away * away, axis=-1, keepdims=True)
        normed = away * lax.rsqrt(spread + epsilon) * head_gain_ref[:, side].astype(f32)
        gate = gate_ref[:, side].astype(f32)
        mixed[:, side] = (jax.nn.silu(gate) * normed).astype(bf16)

    half = count // 2
    give = pl.ds(pl.multiple_of(other * half, half), half)
    keep = pl.ds(pl.multiple_of(c * half, half), half)
    term_out[...] = jnp.dot(
        mixed[give], out_weight_ref[...], preferred_element_type=f32
    ).astype(bf16)
    copy(term_out, term_in, term_sem.at[0], term_sem.at[1], mate).start()
    kept = jnp.dot(mixed[keep], out_weight_ref[...], preferred_element_type=f32)
    residual[...] = stream_ref[...].astype(f32) + kept.astype(bf16).astype(f32)
    arrived(term_in, term_sem.at[1])
    total = residual[...] + term_in[...].astype(f32)
    residual[...] = total
    mean = jnp.mean(total * total, axis=-1, keepdims=True)
    rows[z, c] = (
        total * lax.rsqrt(mean + epsilon) * norm_gain_ref[...].astype(f32)
    ).astype(bf16)

    def pass_on(zz, way):
        copy(
            rows.at[zz, c],
            rows.at[zz, c],
            row_send.at[way, zz],
            row_recv.at[way if way == 0 else 1, zz],
            mate if way == 0 else at(z + 1, n, c) if way == 1 else at(z - 1, n, c),
        ).start()

    def row_step(k):
        @pl.when(z >= k)
        def _():
            arrived(rows.at[z - k, c], row_recv.at[1, z - k])

            @pl.when(z < 3)
            def _():
                pass_on(z - k, 1)

            pass_on(z - k, 0)

        @pl.when(z + k <= 3)
        def _():
            arrived(rows.at[z + k, c], row_recv.at[1, z + k])

            @pl.when(z > 0)
            def _():
                pass_on(z + k, 2)

            pass_on(z + k, 0)

    @pl.when(z < 3)
    def _():
        pass_on(z, 1)

    @pl.when(z > 0)
    def _():
        pass_on(z, 2)

    pass_on(z, 0)

    for kind in (1, 0):
        relay(1, kind)
        push(2, kind)
    row_step(1)
    for kind in (1, 0):
        relay(2, kind)
        push(3, kind)
    row_step(2)
    row_step(3)
    for kind in (1, 0):
        relay(3, kind)
    for kind in (1, 0):
        for d in range(4):
            finish(d, kind)
    for zz in range(4):
        arrived(rows.at[zz, other], row_recv.at[0, zz])

    hidden_size = down.shape[1]
    depth = rows.shape[3]
    ahead = jnp.where(z < 2, 1, 0)

    def block(j, carried):
        zt = j + ahead * (3 - 2 * j)
        x = rows[zt].reshape(count, depth)
        both = jnp.dot(
            x,
            wide[...].reshape(depth, 2 * hidden_size),
            preferred_element_type=f32,
        )
        hidden = (jax.nn.silu(both[:, :hidden_size]) * both[:, hidden_size:]).astype(bf16)
        for p in range(down.shape[0] // 2):
            side = slice(2 * p * down.shape[2], 2 * (p + 1) * down.shape[2])
            pair = jnp.concatenate([down[2 * p], down[2 * p + 1]], axis=1)
            out = jnp.dot(hidden, pair, preferred_element_type=f32).astype(bf16)
            part_own[zt, 0, :, side] = out[:half]
            part_own[zt, 1, :, side] = out[half:]
        copy(
            part_own.at[zt, other], part_in.at[zt], part_sem.at[zt], part_recv.at[zt], mate
        ).start()
        arrived(part_in.at[zt], part_recv.at[zt])

        @pl.when(zt != z)
        def _():
            sum_out[zt] = (
                part_own[zt, c].astype(f32) + part_in[zt].astype(f32)
            ).astype(bf16)
            copy(
                sum_out.at[zt],
                sum_in.at[z],
                sum_send.at[zt],
                sum_recv.at[z],
                at(zt, n, c),
            ).start()

        return carried

    lax.fori_loop(0, 4, block, 0)
    residual[...] += part_own[z, c].astype(f32) + part_in[z].astype(f32)
    for d in (1, 2, 3):
        zz = flip(z, d)
        arrived(sum_in.at[zz], sum_recv.at[zz])
        residual[...] += sum_in[zz].astype(f32)
    result_ref[...] = residual[...].astype(bf16)

    settle_weights()
    for d in (1, 2, 3):
        left(state_out.at[0], st_send.at[d - 1])
        left(entry_out.at[0], en_send.at[d - 1])
        left(sum_out.at[0], sum_send.at[flip(z, d)])

        @pl.when(z + d <= 3)
        def _():
            left(plane_out, pl_send.at[d - 1])

    left(term_out, term_sem.at[0])
    for zz in range(4):
        left(rows.at[0, 0], row_send.at[0, zz])
        left(part_in.at[0], part_sem.at[zz])

        @pl.when((z < 3) & (zz <= z))
        def _():
            left(rows.at[0, 0], row_send.at[1, zz])

        @pl.when((z > 0) & (zz >= z))
        def _():
            left(rows.at[0, 0], row_send.at[2, zz])


def split_total(total, line):
    top = total.astype(bf16).astype(f32)
    mid = (total - top).astype(bf16).astype(f32)
    low = total - top - mid
    return jnp.where(line == 0, top, jnp.where(line == 1, mid, low)).astype(bf16)


def join_total(parts):
    parts = parts.astype(f32)
    return parts[0:1] + parts[1:2] + parts[2:3]


def fused_local(
    stream,
    queries,
    keys_in,
    values_in,
    gate_in,
    log_decay,
    head_gain,
    out_weight,
    norm_gain,
    gate_weight,
    up_weight,
    down_weight,
):
    count, heads = log_decay.shape
    width = queries.shape[1]
    dim = width // heads
    depth = stream.shape[1]
    own, units = gate_weight.shape
    sizes = GROUP * GROUP
    part = units // GROUP
    wide = jnp.concatenate(
        [
            jnp.concatenate(
                [w[:, g * part : (g + 1) * part] for w in (gate_weight, up_weight)], axis=1
            )[None]
            for g in range(GROUP)
        ],
        axis=0,
    )
    down = down_weight.reshape(GROUP, part, down_weight.shape[1])
    half = count // 2
    vmem = pltpu.VMEM
    dma = pltpu.SemaphoreType.DMA
    return pl.pallas_call(
        layer_kernel,
        out_shape=jax.ShapeDtypeStruct((half, depth), bf16),
        in_specs=[pl.BlockSpec(memory_space=vmem)] * 11,
        out_specs=pl.BlockSpec(memory_space=vmem),
        scratch_shapes=[
            vmem((sizes, own, 2 * part), bf16),
            vmem((sizes, part, down_weight.shape[1]), bf16),
            vmem((GROUP, 2, half, depth), bf16),
            vmem((half, depth), f32),
            vmem((count, heads), f32),
            vmem((count, width), f32),
            vmem((heads, dim + TAIL, dim), bf16),
            vmem((heads, dim + TAIL, dim), bf16),
            vmem((dim + TAIL, dim), bf16),
            vmem((GROUP, dim + TAIL, dim), bf16),
            vmem((dim, dim), f32),
            vmem((1, dim), f32),
            vmem((heads, dim, dim), bf16),
            vmem((heads, dim, dim), bf16),
            vmem((count, width), bf16),
            vmem((half, depth), bf16),
            vmem((half, depth), bf16),
            vmem((16, 128), bf16),
            vmem((GROUP, 2, half, depth), bf16),
            vmem((GROUP, half, depth), bf16),
            vmem((GROUP, half, depth), bf16),
            vmem((GROUP, half, depth), bf16),
            dma((2, GROUP, 2)),
            dma((2, GROUP, 2)),
            dma((2, sizes, 2)),
            dma((2, GROUP - 1)),
            dma((3,)),
            dma((3,)),
            dma((3,)),
            dma((GROUP,)),
            dma((3,)),
            dma((3,)),
            dma((2,)),
            dma((3, GROUP)),
            dma((2, GROUP)),
            dma((GROUP,)),
            dma((GROUP,)),
            dma((GROUP,)),
            dma((GROUP,)),
        ],
        compiler_params=pltpu.CompilerParams(
            collective_id=0, has_side_effects=True, vmem_limit_bytes=60 * 1024 * 1024
        ),
        name="layer",
    )(
        stream,
        queries,
        keys_in,
        values_in,
        gate_in,
        log_decay,
        head_gain[None],
        out_weight,
        norm_gain[None],
        wide,
        down,
    )


def fused(mesh):
    return jax.shard_map(
        fused_local,
        mesh=mesh,
        in_specs=(
            P(("sp", "tp"), None),
            P("sp", "tp"),
            P("sp", "tp"),
            P("sp", "tp"),
            P("sp", "tp"),
            P("sp", "tp"),
            P("tp"),
            P("tp", None),
            P(),
            P("sp", "tp"),
            P("sp", "tp"),
            P("tp", "sp"),
        ),
        out_specs=P(("sp", "tp"), None),
        check_vma=False,
    )


def solution(mesh):
    if fits(mesh):
        return fused(mesh)
    devices = mesh.devices
    count, pair = devices.shape
    split = Mesh(devices.reshape(GROUP, count // GROUP, pair), (*SP, "tp"))
    return jax.shard_map(
        local,
        mesh=split,
        in_specs=(
            P((*SP, "tp"), None),
            P(SP, "tp"),
            P(SP, "tp"),
            P(SP, "tp"),
            P(SP, "tp"),
            P(SP, "tp"),
            P("tp"),
            P("tp", None),
            P(),
            P(SP, "tp"),
            P(SP, "tp"),
            P("tp", SP),
        ),
        out_specs=P((*SP, "tp"), None),
        check_vma=False,
    )
```

```python
import functools

import jax
import jax.numpy as jnp
from jax import lax
from jax.experimental import pallas as pl
from jax.experimental.pallas import tpu as pltpu
from jax.sharding import Mesh, PartitionSpec as P

epsilon = 1e-06
GROUP = 4
SP = ("far", "near")
f32, bf16 = jnp.float32, jnp.bfloat16


def swap(value, axis, bits):
    size = lax.axis_size(axis)
    return lax.ppermute(value, axis, [(i, i ^ bits) for i in range(size)])


def near_blocks(value):
    size = lax.axis_size("near")
    steps = (1, 2) if size == 4 else range(1, size)
    return [value] + [swap(value, "near", s) for s in steps]


def near_rest(blocks):
    half = blocks[0].shape[0] // 2
    cut = [(block[:half], block[half:]) for block in blocks]
    if lax.axis_size("near") == 4:
        cut.append((swap(cut[1][0], "near", 2), swap(cut[2][1], "near", 1)))
    return cut


def spread_weights(gate_weight, up_weight, down_weight):
    groups = lax.axis_size("far")
    far_at = lax.axis_index("far")
    width = gate_weight.shape[1] // groups
    all_rows, all_columns = [], []
    for s in range(groups):
        at = (far_at ^ s) * width
        rows = jnp.concatenate(
            [
                lax.dynamic_slice_in_dim(gate_weight, at, width, 1),
                lax.dynamic_slice_in_dim(up_weight, at, width, 1),
            ],
            axis=0,
        )
        all_rows.append(swap(rows, "far", s) if s else rows)
    for s in range(groups):
        at = (far_at ^ s) * width
        all_columns.append(lax.dynamic_slice_in_dim(down_weight, at, width, 0))
    return [near_blocks(piece) for piece in all_rows], all_columns


def by_distance(value):
    groups, near = lax.axis_size("far"), lax.axis_size("near")
    here = lax.axis_index("far") * near + lax.axis_index("near")
    width = value.shape[1] // (groups * near)
    return jnp.concatenate(
        [
            lax.dynamic_slice_in_dim(value, (here ^ k) * width, width, 1)
            for k in range(groups * near)
        ],
        axis=1,
    )


def turned(value, bits):
    groups = lax.axis_size("far")
    width = value.shape[1] // groups
    return jnp.concatenate(
        [value[:, (g ^ bits) * width : ((g ^ bits) + 1) * width] for g in range(groups)], axis=1
    )


def gather_pair(rows):
    if lax.axis_size("tp") == 2:
        return jnp.concatenate([rows, swap(rows, "tp", 1)], axis=0)
    return lax.all_gather(rows, "tp", axis=0, tiled=True)


def scatter_pair(terms):
    terms = terms.astype(bf16)
    if lax.axis_size("tp") == 2:
        half = terms.shape[0] // 2
        return terms[:half].astype(f32) + swap(terms[half:], "tp", 1).astype(f32)
    return lax.psum_scatter(terms, "tp", scatter_dimension=0, tiled=True).astype(f32)


def dot(a, b, dims=((1,), (0,))):
    return lax.dot_general(a, b, (dims, ((), ())), preferred_element_type=f32)


def retention(queries, keys_in, values_in, log_decay):
    row_count, heads = log_decay.shape
    dim = queries.shape[1] // heads
    scale = dim ** (-0.5)
    running = jnp.cumsum(log_decay, axis=0)
    total = running[-1]
    offsets = jnp.arange(row_count)
    causal = offsets[:, None] >= offsets[None, :]
    within, states = [], []
    for h in range(heads):
        cut = slice(h * dim, (h + 1) * dim)
        q, k, v = queries[:, cut], keys_in[:, cut], values_in[:, cut]
        col = running[:, h]
        gap = jnp.minimum(col[:, None] - col[None, :], 0.0)
        table = jnp.where(causal, jnp.exp(gap), 0.0) * scale
        within.append(dot((dot(q, k, ((1,), (1,))) * table).astype(bf16), v))
        tail = (jnp.exp(total[h] - col) * scale)[:, None]
        states.append(dot((k.astype(f32) * tail).astype(bf16), v, ((0,), (0,))))
    return running, total, within, jnp.concatenate(states, axis=0)


def incoming_states(total, state, columns):
    heads = total.shape[0]
    near = lax.axis_size("near")
    here = lax.axis_index("far") * near + lax.axis_index("near")
    high = lax.reduce_precision(total, 8, 7)
    mid = lax.reduce_precision(total - high, 8, 7)
    low = total - high - mid
    parts = jnp.concatenate([high, mid, low])
    extra = -(-parts.shape[0] // 16) * 16
    parts = jnp.pad(parts, (0, extra - parts.shape[0]))
    width = state.shape[1]
    packed = jnp.concatenate(
        [state.astype(bf16), jnp.broadcast_to(parts[:, None], (extra, width)).astype(bf16)], axis=0
    )
    everything = lax.all_gather(packed, SP)
    everything, columns = lax.optimization_barrier((everything, columns))
    columns = [swap(piece, "far", s) if s else piece for s, piece in enumerate(columns)]
    count = everything.shape[0]
    logs = everything[:, state.shape[0] : state.shape[0] + 3 * heads, 0].astype(f32)
    logs = logs.reshape(count, 3, heads).sum(axis=1)
    index = jnp.arange(count)
    between = (index[None, :] > index[:, None]) & (index[None, :] < here)
    reach = jnp.sum(jnp.where(between[:, :, None], logs[None], 0.0), axis=1)
    factor = jnp.where((index < here)[:, None], jnp.exp(reach), 0.0)
    states = everything[:, : state.shape[0]].reshape(count, heads, -1, width)
    return jnp.sum(factor[:, :, None, None] * states.astype(f32), axis=0), columns


def local(
    stream,
    queries,
    keys_in,
    values_in,
    gate_in,
    log_decay,
    head_gain,
    out_weight,
    norm_gain,
    gate_weight,
    up_weight,
    down_weight,
):
    weight_rows, weight_columns = spread_weights(gate_weight, up_weight, down_weight)
    heads = log_decay.shape[1]
    dim = queries.shape[1] // heads
    running, total, within, state = retention(queries, keys_in, values_in, log_decay)
    incoming, weight_columns = incoming_states(total, state, weight_columns)
    mixed = []
    for h in range(heads):
        cut = slice(h * dim, (h + 1) * dim)
        carried = dot(queries[:, cut], incoming[h].astype(bf16))
        retained = within[h] + carried * jnp.exp(running[:, h])[:, None]
        center = jnp.mean(retained, axis=-1, keepdims=True)
        spread = jnp.mean(jnp.square(retained - center), axis=-1, keepdims=True)
        normed = (retained - center) * lax.rsqrt(spread + epsilon) * head_gain[cut].astype(f32)
        mixed.append((jax.nn.silu(gate_in[:, cut].astype(f32)) * normed).astype(bf16))
    terms = dot(jnp.concatenate(mixed, axis=1), out_weight).astype(bf16)
    if lax.axis_size("tp") == 2:
        half = terms.shape[0] // 2
        mine = lax.axis_index("tp") * half
        sent = swap(lax.dynamic_slice_in_dim(terms, half - mine, half, 0), "tp", 1)
        kept = lax.dynamic_slice_in_dim(terms, mine, half, 0)
        attended = kept.astype(f32) + sent.astype(f32)
    else:
        attended = scatter_pair(terms)
    residual = stream.astype(f32) + attended
    normed = (
        residual
        * lax.rsqrt(jnp.mean(residual * residual, axis=-1, keepdims=True) + epsilon)
        * norm_gain.astype(f32)
    ).astype(bf16)

    normed = by_distance(normed)
    normed, weight_rows, weight_columns = lax.optimization_barrier(
        (normed, weight_rows, weight_columns)
    )
    weight_rows = [block for piece in weight_rows for block in near_rest(piece)]
    weight_columns = [
        block for piece in weight_columns for block in near_rest(near_blocks(piece))
    ]
    groups = lax.axis_size("far")
    arrived = [normed] + [swap(normed, "far", s) for s in range(1, groups)]
    rows = [turned(gather_pair(piece), s) for s, piece in enumerate(arrived)]
    gate_full = jnp.concatenate([gate for gate, _ in weight_rows], axis=0)
    up_full = jnp.concatenate([up for _, up in weight_rows], axis=0)
    down_full = jnp.concatenate(
        [jnp.concatenate([part[i] for part in weight_columns], axis=1) for i in range(2)], axis=0
    )
    together = jnp.concatenate(rows, axis=0)
    hidden = (jax.nn.silu(dot(together, gate_full)) * dot(together, up_full)).astype(bf16)
    height = rows[0].shape[0]
    mixer_out = 0.0
    for s in (*range(1, groups), 0):
        part = scatter_pair(dot(hidden[s * height : (s + 1) * height], down_full))
        if s:
            part = turned(swap(part.astype(bf16), "far", s).astype(f32), s)
        mixer_out = mixer_out + part
    return (residual + by_distance(mixer_out)).astype(bf16)


MESH = pl.DeviceIdType.MESH
HIGHEST = lax.Precision.HIGHEST
TAIL = 16
PIECES = 2


def fits(mesh):
    return mesh.shape["tp"] == 2 and mesh.shape["sp"] == GROUP * GROUP


def flip(v, d):
    if d == 0:
        return v
    if d == 1:
        return v + 1 - 2 * lax.rem(v, 2)
    if d == 2:
        return lax.rem(v + 2, 4)
    return 3 - v


def layer_kernel(
    stream_in,
    q_in,
    k_in,
    v_in,
    gate_in,
    decay_in,
    head_gain_in,
    out_weight_in,
    norm_gain_in,
    gate_weight_in,
    up_weight_in,
    down_in,
    result_ref,
    stream_ref,
    q_ref,
    k_ref,
    v_ref,
    gate_ref,
    decay_ref,
    head_gain_ref,
    out_weight_ref,
    norm_gain_ref,
    gate_weight_ref,
    up_weight_ref,
    wide_own,
    wide,
    down,
    rows,
    residual,
    grown,
    within,
    state_out,
    state_in,
    plane_out,
    plane_in,
    carry,
    reach,
    entry_out,
    entry_in,
    mixed,
    term_out,
    term_in,
    part_own,
    part_in,
    sum_own,
    sum_out,
    sum_in,
    in_sem,
    w_send,
    w_relay,
    w_recv,
    w_far,
    st_send,
    st_recv,
    pl_send,
    pl_recv,
    en_send,
    en_recv,
    term_sem,
    row_send,
    row_recv,
    part_sem,
    part_recv,
    sum_send,
    sum_recv,
):
    sp, c = lax.axis_index("sp"), lax.axis_index("tp")
    z, n = lax.div(sp, 4), lax.rem(sp, 4)
    other = 1 - c
    beside = [flip(n, d) for d in range(4)]
    inner = jnp.where(z < 2, 1, -1)
    middle = (z == 1) | (z == 2)
    edge = (z == 0) | (z == 3)
    level = [
        z,
        flip(z, 1),
        jnp.where(edge, flip(z, 2), flip(z, 3)),
        jnp.where(edge, flip(z, 3), flip(z, 2)),
    ]

    def at(zz, nn, cc):
        return (zz * 4 + nn, cc)

    mate = at(z, n, other)

    def copy(src, dst, send, recv, to):
        return pltpu.make_async_remote_copy(
            src_ref=src,
            dst_ref=dst,
            send_sem=send,
            recv_sem=recv,
            device_id=to,
            device_id_type=MESH,
        )

    def arrived(ref, recv):
        copy(ref, ref, recv, recv, mate).wait_recv()

    def left(ref, send):
        copy(ref, ref, send, send, mate).wait_send()

    loads = [
        pltpu.make_async_copy(src, dst, in_sem.at[i])
        for i, (src, dst) in enumerate(
            (
                (gate_weight_in, gate_weight_ref),
                (up_weight_in, up_weight_ref),
                (decay_in, decay_ref),
                (k_in, k_ref),
                (v_in, v_ref),
                (q_in, q_ref),
                (down_in.at[z], down.at[sp]),
                (gate_in, gate_ref),
                (head_gain_in, head_gain_ref),
                (out_weight_in, out_weight_ref),
                (stream_in, stream_ref),
                (norm_gain_in, norm_gain_ref),
            )
        )
    ]
    for load in loads:
        load.start()

    barrier = pltpu.get_barrier_semaphore()
    partners = [mate]
    partners += [at(z, beside[d], c) for d in (1, 2, 3)]
    partners += [at(flip(z, d), n, c) for d in (1, 2, 3)]
    for to in partners:
        pl.semaphore_signal(barrier, inc=1, device_id=to, device_id_type=MESH)

    units = down.shape[1]
    loads[0].wait()
    loads[1].wait()
    for g in range(wide_own.shape[0]):
        side = slice(g * units, (g + 1) * units)
        wide_own[g] = jnp.concatenate(
            [gate_weight_ref[:, side], up_weight_ref[:, side]], axis=1
        )
    pl.semaphore_wait(barrier, len(partners))

    full = (wide, down)
    given = (wide_own, down_in)
    cut = (wide.shape[1] // 2, down.shape[1] // 2)

    def far(d, kind):
        copy(
            given[kind].at[level[d]],
            full[kind].at[sp],
            w_far.at[kind, d - 1],
            w_recv.at[kind, sp, 0],
            at(level[d], n, c),
        ).start()

    def push(d, kind):
        slot = level[d] * 4 + n
        if d:
            arrived(full[kind].at[slot], w_recv.at[kind, slot, 0])
        src = full[kind].at[slot] if d else given[kind].at[z]
        for a in (1, 2):
            copy(
                src,
                full[kind].at[slot],
                w_send.at[kind, d, a - 1],
                w_recv.at[kind, slot, 0],
                at(z, beside[a], c),
            ).start()

    def relay(d, kind):
        half = cut[kind]
        for a in (1, 2):
            slot = level[d] * 4 + beside[a]
            arrived(full[kind].at[slot], w_recv.at[kind, slot, 0])
            part = pl.ds(0, half) if a == 1 else pl.ds(half, half)
            piece = full[kind].at[slot, part]
            copy(
                piece,
                piece,
                w_relay.at[kind, d, a - 1],
                w_recv.at[kind, slot, a - 1],
                at(z, beside[3 - a], c),
            ).start()

    def finish(d, kind):
        half = cut[kind]
        slot = level[d] * 4 + beside[3]
        arrived(full[kind].at[slot, pl.ds(0, half)], w_recv.at[kind, slot, 0])
        arrived(full[kind].at[slot, pl.ds(half, half)], w_recv.at[kind, slot, 1])

    def settle_weights():
        for kind in (0, 1):
            half = cut[kind]
            for d in range(4):
                if d:
                    left(given[kind].at[0], w_far.at[kind, d - 1])
                for a in (0, 1):
                    left(given[kind].at[0], w_send.at[kind, d, a])
                    left(full[kind].at[0, pl.ds(0, half)], w_relay.at[kind, d, a])

    push(0, 1)
    far(1, 1)

    @pl.when(middle)
    def _():
        far(2, 1)

    heads = decay_ref.shape[0]
    dim = q_ref.shape[1] // heads
    count = q_ref.shape[0]
    scale = dim ** (-0.5)
    loads[2].wait()
    decay = decay_ref[...]
    low = lax.broadcasted_iota(jnp.int32, (count, count), 0)
    high = lax.broadcasted_iota(jnp.int32, (count, count), 1)
    causal = low >= high
    running = jnp.dot(
        decay, (low <= high).astype(f32), precision=HIGHEST, preferred_element_type=f32
    )
    line = lax.broadcasted_iota(jnp.int32, (TAIL, dim), 0)
    loads[3].wait()
    loads[4].wait()
    cols = []
    for h in range(heads):
        side = slice(h * dim, (h + 1) * dim)
        col = jnp.broadcast_to(running[h : h + 1], (dim, count)).T
        cols.append(col)
        total = running[h : h + 1, count - 1 : count]
        tail = jnp.exp(total - col) * scale
        keyed = (k_ref[:, side].astype(f32) * tail).T.astype(bf16)
        state = jnp.dot(keyed, v_ref[:, side], preferred_element_type=f32)
        state_out[h, :dim] = state.astype(bf16)
        state_out[h, dim:] = split_total(total, line)

    for d in (1, 2, 3):
        copy(
            state_out.at[beside[d]],
            state_in.at[n],
            st_send.at[d - 1],
            st_recv.at[d - 1],
            at(z, beside[d], c),
        ).start()
    state_in[n] = state_out[n]
    push(0, 0)
    far(1, 0)

    @pl.when(middle)
    def _():
        far(2, 0)

    wide[sp] = wide_own[z]

    for d in (1, 2, 3):
        arrived(state_in.at[beside[d]], st_recv.at[d - 1])
    totals = [join_total(state_in[m, dim:]) for m in range(4)]
    states = [state_in[m, :dim].astype(f32) for m in range(4)]
    plane, span = states[0], totals[0]
    for m in range(1, 4):
        plane = plane * jnp.exp(totals[m]) + states[m]
        span = span + totals[m]
    plane_out[:dim] = plane.astype(bf16)
    plane_out[dim:] = split_total(span, line)
    for k in (1, 2, 3):

        @pl.when(z + k <= 3)
        def _():
            copy(
                plane_out,
                plane_in.at[z],
                pl_send.at[k - 1],
                pl_recv.at[z],
                at(z + k, n, c),
            ).start()

    @pl.when(edge)
    def _():
        far(2, 1)
        far(2, 0)

    far(3, 1)
    far(3, 0)

    loads[5].wait()
    for h in range(heads):
        side = slice(h * dim, (h + 1) * dim)
        q, k, v = q_ref[:, side], k_ref[:, side], v_ref[:, side]
        gap = jnp.minimum(cols[h][:, :1] - running[h : h + 1], 0.0)
        table = jnp.where(causal, jnp.exp(gap), 0.0) * scale
        scores = dot(q, k, ((1,), (1,)))
        within[:, side] = jnp.dot(
            (scores * table).astype(bf16), v, preferred_element_type=f32
        )
        grown[h] = jnp.exp(cols[h])

    carry[...] = jnp.zeros_like(carry)
    reach[...] = jnp.zeros_like(reach)
    for k in (1, 2, 3):

        @pl.when(z >= k)
        def _():
            arrived(plane_in.at[z - k], pl_recv.at[z - k])
            carry[...] += jnp.exp(reach[...]) * plane_in[z - k, :dim].astype(f32)
            reach[...] += join_total(plane_in[z - k, dim:])

    entry = carry[...]
    for m in range(4):
        entry_out[m] = entry.astype(bf16)
        if m < 3:
            entry = entry * jnp.exp(totals[m]) + states[m]
    for d in (1, 2, 3):
        copy(
            entry_out.at[beside[d]],
            entry_in.at[n],
            en_send.at[d - 1],
            en_recv.at[d - 1],
            at(z, beside[d], c),
        ).start()
    entry_in[n] = entry_out[n]

    for kind in (1, 0):
        relay(0, kind)
        push(1, kind)

    for d in (1, 2, 3):
        arrived(entry_in.at[beside[d]], en_recv.at[d - 1])
    for load in loads[6:]:
        load.wait()
    for h in range(heads):
        side = slice(h * dim, (h + 1) * dim)
        carried = jnp.dot(q_ref[:, side], entry_in[h], preferred_element_type=f32)
        retained = within[:, side] + carried * grown[h]
        center = jnp.mean(retained, axis=-1, keepdims=True)
        away = retained - center
        spread = jnp.mean(away * away, axis=-1, keepdims=True)
        normed = away * lax.rsqrt(spread + epsilon) * head_gain_ref[:, side].astype(f32)
        gate = gate_ref[:, side].astype(f32)
        mixed[:, side] = (jax.nn.silu(gate) * normed).astype(bf16)

    half = count // 2
    give = pl.ds(pl.multiple_of(other * half, half), half)
    keep = pl.ds(pl.multiple_of(c * half, half), half)
    term_out[...] = jnp.dot(
        mixed[give], out_weight_ref[...], preferred_element_type=f32
    ).astype(bf16)
    copy(term_out, term_in, term_sem.at[0], term_sem.at[1], mate).start()
    kept = jnp.dot(mixed[keep], out_weight_ref[...], preferred_element_type=f32)
    residual[...] = stream_ref[...].astype(f32) + kept.astype(bf16).astype(f32)
    arrived(term_in, term_sem.at[1])
    total = residual[...] + term_in[...].astype(f32)
    residual[...] = total
    mean = jnp.mean(total * total, axis=-1, keepdims=True)
    rows[z, c] = (
        total * lax.rsqrt(mean + epsilon) * norm_gain_ref[...].astype(f32)
    ).astype(bf16)

    pieces = PIECES
    high = half // pieces

    def strip(p):
        return pl.ds(p * high, high)

    def pass_on(zz, way, p):
        piece = rows.at[zz, c, strip(p)]
        copy(
            piece,
            piece,
            row_send.at[way, zz, p],
            row_recv.at[min(way, 1), zz, p],
            (mate, at(z + inner, n, c), at(z - inner, n, c))[way],
        ).start()

    def from_outer():
        @pl.when(middle)
        def _():
            zz = z - inner
            for p in range(pieces):
                arrived(rows.at[zz, c, strip(p)], row_recv.at[1, zz, p])
                pass_on(zz, 1, p)
                pass_on(zz, 0, p)

    def from_inner(k):
        def go():
            zz = z + inner * k
            for p in range(pieces):
                arrived(rows.at[zz, c, strip(p)], row_recv.at[1, zz, p])
                if k < 3:

                    @pl.when(middle)
                    def _():
                        pass_on(zz, 2, p)

                pass_on(zz, 0, p)

        if k < 3:
            go()
        else:
            pl.when(edge)(go)

    for p in range(pieces):
        pass_on(z, 1, p)

        @pl.when(middle)
        def _():
            pass_on(z, 2, p)

        pass_on(z, 0, p)

    for kind in (1, 0):
        relay(1, kind)
        push(2, kind)
    from_outer()
    for kind in (1, 0):
        relay(2, kind)
        push(3, kind)
    from_inner(1)
    for kind in (1, 0):
        relay(3, kind)
    from_inner(2)
    from_inner(3)
    for kind in (1, 0):
        for d in range(4):
            finish(d, kind)

    depth = rows.shape[3]

    def turn(j):
        away = jnp.where(j == 0, 2, jnp.where(j == 1, -1, jnp.where(j == 2, 1, 0)))
        return z + inner * jnp.where(edge, 3 - j, away)

    def send_sum(zt, p, to, side):
        copy(
            sum_out.at[zt, strip(p)],
            sum_in.at[side, zt, strip(p)],
            sum_send.at[zt, p],
            sum_recv.at[side, zt, p],
            to,
        ).start()

    def gather(zt):
        arrived(part_in.at[zt], part_recv.at[zt])
        sum_own[zt] = part_own[zt, c].astype(f32) + part_in[zt].astype(f32)

        @pl.when(edge & (zt != z))
        def _():
            sum_out[zt] = sum_own[zt].astype(bf16)
            for p in range(pieces):
                send_sum(zt, p, at(z + inner, n, c), 0)

    def block(j, carried):
        zt = turn(j)
        for p in range(pieces):
            arrived(rows.at[zt, other, strip(p)], row_recv.at[0, zt, p])
        x = rows[zt].reshape(count, depth)
        both = jnp.dot(
            x,
            wide[...].reshape(depth, 2 * units),
            preferred_element_type=f32,
        )
        hidden = (jax.nn.silu(both[:, :units]) * both[:, units:]).astype(bf16)
        for p in range(down.shape[0] // 2):
            side = slice(2 * p * down.shape[2], 2 * (p + 1) * down.shape[2])
            pair = jnp.concatenate([down[2 * p], down[2 * p + 1]], axis=1)
            out = jnp.dot(hidden, pair, preferred_element_type=f32).astype(bf16)
            part_own[zt, 0, :, side] = out[:half]
            part_own[zt, 1, :, side] = out[half:]
        copy(
            part_own.at[zt, other], part_in.at[zt], part_sem.at[zt], part_recv.at[zt], mate
        ).start()

        @pl.when(j > 0)
        def _():
            gather(turn(j - 1))

        return carried

    lax.fori_loop(0, GROUP, block, 0)
    gather(z)

    def add_on(zt, side, to):
        for p in range(pieces):
            arrived(sum_in.at[side, zt, strip(p)], sum_recv.at[side, zt, p])
            sum_out[zt, strip(p)] = (
                sum_own[zt, strip(p)] + sum_in[side, zt, strip(p)].astype(f32)
            ).astype(bf16)
            send_sum(zt, p, to, 1)

    @pl.when(middle)
    def _():
        add_on(z + 2 * inner, 0, at(z + inner, n, c))
        add_on(z - inner, 1, at(z - inner, n, c))
        add_on(z + inner, 0, at(z + inner, n, c))

    residual[...] += sum_own[z]

    @pl.when(middle)
    def _():
        for p in range(pieces):
            arrived(sum_in.at[0, z, strip(p)], sum_recv.at[0, z, p])
            residual[strip(p)] += sum_in[0, z, strip(p)].astype(f32)

    for p in range(pieces):
        arrived(sum_in.at[1, z, strip(p)], sum_recv.at[1, z, p])
        result_ref[strip(p)] = (
            residual[strip(p)] + sum_in[1, z, strip(p)].astype(f32)
        ).astype(result_ref.dtype)

    settle_weights()
    for d in (1, 2, 3):
        left(state_out.at[0], st_send.at[d - 1])
        left(entry_out.at[0], en_send.at[d - 1])
        for p in range(pieces):
            left(sum_out.at[0, strip(0)], sum_send.at[flip(z, d), p])

        @pl.when(z + d <= 3)
        def _():
            left(plane_out, pl_send.at[d - 1])

    left(term_out, term_sem.at[0])
    for zz in range(GROUP):
        left(part_in.at[0], part_sem.at[zz])
        for p in range(pieces):
            left(rows.at[0, 0, strip(0)], row_send.at[0, zz, p])
    for p in range(pieces):
        left(rows.at[0, 0, strip(0)], row_send.at[1, z, p])

        @pl.when(middle)
        def _():
            left(rows.at[0, 0, strip(0)], row_send.at[1, z - inner, p])
            for k in range(3):
                left(rows.at[0, 0, strip(0)], row_send.at[2, z + inner * k, p])


def split_total(total, line):
    top = total.astype(bf16).astype(f32)
    mid = (total - top).astype(bf16).astype(f32)
    low = total - top - mid
    return jnp.where(line == 0, top, jnp.where(line == 1, mid, low)).astype(bf16)


def join_total(parts):
    parts = parts.astype(f32)
    return parts[0:1] + parts[1:2] + parts[2:3]


def fused_local(
    stream,
    queries,
    keys_in,
    values_in,
    gate_in,
    log_decay,
    head_gain,
    out_weight,
    norm_gain,
    gate_weight,
    up_weight,
    down_weight,
):
    count, heads = log_decay.shape
    width = queries.shape[1]
    dim = width // heads
    depth = stream.shape[1]
    own, units = gate_weight.shape
    sizes = GROUP * GROUP
    part = units // GROUP
    down = down_weight.reshape(GROUP, part, down_weight.shape[1])
    half = count // 2
    vmem = pltpu.VMEM
    dma = pltpu.SemaphoreType.DMA
    given = (
        stream,
        queries,
        keys_in,
        values_in,
        gate_in,
        log_decay.T,
        head_gain[None],
        out_weight,
        norm_gain[None],
        gate_weight,
        up_weight,
    )
    return pl.pallas_call(
        layer_kernel,
        out_shape=jax.ShapeDtypeStruct((half, depth), bf16),
        in_specs=[pl.BlockSpec(memory_space=pl.ANY)] * 12,
        out_specs=pl.BlockSpec(memory_space=vmem),
        scratch_shapes=[
            *(vmem(value.shape, value.dtype) for value in given),
            vmem((GROUP, own, 2 * part), bf16),
            vmem((sizes, own, 2 * part), bf16),
            vmem((sizes, part, down_weight.shape[1]), bf16),
            vmem((GROUP, 2, half, depth), bf16),
            vmem((half, depth), f32),
            vmem((heads, count, dim), f32),
            vmem((count, width), f32),
            vmem((heads, dim + TAIL, dim), bf16),
            vmem((heads, dim + TAIL, dim), bf16),
            vmem((dim + TAIL, dim), bf16),
            vmem((GROUP, dim + TAIL, dim), bf16),
            vmem((dim, dim), f32),
            vmem((1, dim), f32),
            vmem((heads, dim, dim), bf16),
            vmem((heads, dim, dim), bf16),
            vmem((count, width), bf16),
            vmem((half, depth), bf16),
            vmem((half, depth), bf16),
            vmem((GROUP, 2, half, depth), bf16),
            vmem((GROUP, half, depth), bf16),
            vmem((GROUP, half, depth), f32),
            vmem((GROUP, half, depth), bf16),
            vmem((2, GROUP, half, depth), bf16),
            dma((12,)),
            dma((2, GROUP, 2)),
            dma((2, GROUP, 2)),
            dma((2, sizes, 2)),
            dma((2, GROUP - 1)),
            dma((3,)),
            dma((3,)),
            dma((3,)),
            dma((GROUP,)),
            dma((3,)),
            dma((3,)),
            dma((2,)),
            dma((3, GROUP, PIECES)),
            dma((2, GROUP, PIECES)),
            dma((GROUP,)),
            dma((GROUP,)),
            dma((GROUP, PIECES)),
            dma((2, GROUP, PIECES)),
        ],
        compiler_params=pltpu.CompilerParams(
            collective_id=0, has_side_effects=True, vmem_limit_bytes=60 * 1024 * 1024
        ),
        name="layer",
    )(*given, down)


def fused(mesh):
    return jax.shard_map(
        fused_local,
        mesh=mesh,
        in_specs=(
            P(("sp", "tp"), None),
            P("sp", "tp"),
            P("sp", "tp"),
            P("sp", "tp"),
            P("sp", "tp"),
            P("sp", "tp"),
            P("tp"),
            P("tp", None),
            P(),
            P("sp", "tp"),
            P("sp", "tp"),
            P("tp", "sp"),
        ),
        out_specs=P(("sp", "tp"), None),
        check_vma=False,
    )


def solution(mesh):
    if fits(mesh):
        return fused(mesh)
    devices = mesh.devices
    count, pair = devices.shape
    split = Mesh(devices.reshape(GROUP, count // GROUP, pair), (*SP, "tp"))
    return jax.shard_map(
        local,
        mesh=split,
        in_specs=(
            P((*SP, "tp"), None),
            P(SP, "tp"),
            P(SP, "tp"),
            P(SP, "tp"),
            P(SP, "tp"),
            P(SP, "tp"),
            P("tp"),
            P("tp", None),
            P(),
            P(SP, "tp"),
            P(SP, "tp"),
            P("tp", SP),
        ),
        out_specs=P((*SP, "tp"), None),
        check_vma=False,
    )
```

```python
import functools

import jax
import jax.numpy as jnp
from jax import lax
from jax.experimental import pallas as pl
from jax.experimental.pallas import tpu as pltpu
from jax.sharding import Mesh, PartitionSpec as P

epsilon = 1e-06
GROUP = 4
SP = ("far", "near")
f32, bf16 = jnp.float32, jnp.bfloat16


def swap(value, axis, bits):
    size = lax.axis_size(axis)
    return lax.ppermute(value, axis, [(i, i ^ bits) for i in range(size)])


def near_blocks(value):
    size = lax.axis_size("near")
    steps = (1, 2) if size == 4 else range(1, size)
    return [value] + [swap(value, "near", s) for s in steps]


def near_rest(blocks):
    half = blocks[0].shape[0] // 2
    cut = [(block[:half], block[half:]) for block in blocks]
    if lax.axis_size("near") == 4:
        cut.append((swap(cut[1][0], "near", 2), swap(cut[2][1], "near", 1)))
    return cut


def spread_weights(gate_weight, up_weight, down_weight):
    groups = lax.axis_size("far")
    far_at = lax.axis_index("far")
    width = gate_weight.shape[1] // groups
    all_rows, all_columns = [], []
    for s in range(groups):
        at = (far_at ^ s) * width
        rows = jnp.concatenate(
            [
                lax.dynamic_slice_in_dim(gate_weight, at, width, 1),
                lax.dynamic_slice_in_dim(up_weight, at, width, 1),
            ],
            axis=0,
        )
        all_rows.append(swap(rows, "far", s) if s else rows)
    for s in range(groups):
        at = (far_at ^ s) * width
        all_columns.append(lax.dynamic_slice_in_dim(down_weight, at, width, 0))
    return [near_blocks(piece) for piece in all_rows], all_columns


def by_distance(value):
    groups, near = lax.axis_size("far"), lax.axis_size("near")
    here = lax.axis_index("far") * near + lax.axis_index("near")
    width = value.shape[1] // (groups * near)
    return jnp.concatenate(
        [
            lax.dynamic_slice_in_dim(value, (here ^ k) * width, width, 1)
            for k in range(groups * near)
        ],
        axis=1,
    )


def turned(value, bits):
    groups = lax.axis_size("far")
    width = value.shape[1] // groups
    return jnp.concatenate(
        [value[:, (g ^ bits) * width : ((g ^ bits) + 1) * width] for g in range(groups)], axis=1
    )


def gather_pair(rows):
    if lax.axis_size("tp") == 2:
        return jnp.concatenate([rows, swap(rows, "tp", 1)], axis=0)
    return lax.all_gather(rows, "tp", axis=0, tiled=True)


def scatter_pair(terms):
    terms = terms.astype(bf16)
    if lax.axis_size("tp") == 2:
        half = terms.shape[0] // 2
        return terms[:half].astype(f32) + swap(terms[half:], "tp", 1).astype(f32)
    return lax.psum_scatter(terms, "tp", scatter_dimension=0, tiled=True).astype(f32)


def dot(a, b, dims=((1,), (0,))):
    return lax.dot_general(a, b, (dims, ((), ())), preferred_element_type=f32)


def retention(queries, keys_in, values_in, log_decay):
    row_count, heads = log_decay.shape
    dim = queries.shape[1] // heads
    scale = dim ** (-0.5)
    running = jnp.cumsum(log_decay, axis=0)
    total = running[-1]
    offsets = jnp.arange(row_count)
    causal = offsets[:, None] >= offsets[None, :]
    within, states = [], []
    for h in range(heads):
        cut = slice(h * dim, (h + 1) * dim)
        q, k, v = queries[:, cut], keys_in[:, cut], values_in[:, cut]
        col = running[:, h]
        gap = jnp.minimum(col[:, None] - col[None, :], 0.0)
        table = jnp.where(causal, jnp.exp(gap), 0.0) * scale
        within.append(dot((dot(q, k, ((1,), (1,))) * table).astype(bf16), v))
        tail = (jnp.exp(total[h] - col) * scale)[:, None]
        states.append(dot((k.astype(f32) * tail).astype(bf16), v, ((0,), (0,))))
    return running, total, within, jnp.concatenate(states, axis=0)


def incoming_states(total, state, columns):
    heads = total.shape[0]
    near = lax.axis_size("near")
    here = lax.axis_index("far") * near + lax.axis_index("near")
    high = lax.reduce_precision(total, 8, 7)
    mid = lax.reduce_precision(total - high, 8, 7)
    low = total - high - mid
    parts = jnp.concatenate([high, mid, low])
    extra = -(-parts.shape[0] // 16) * 16
    parts = jnp.pad(parts, (0, extra - parts.shape[0]))
    width = state.shape[1]
    packed = jnp.concatenate(
        [state.astype(bf16), jnp.broadcast_to(parts[:, None], (extra, width)).astype(bf16)], axis=0
    )
    everything = lax.all_gather(packed, SP)
    everything, columns = lax.optimization_barrier((everything, columns))
    columns = [swap(piece, "far", s) if s else piece for s, piece in enumerate(columns)]
    count = everything.shape[0]
    logs = everything[:, state.shape[0] : state.shape[0] + 3 * heads, 0].astype(f32)
    logs = logs.reshape(count, 3, heads).sum(axis=1)
    index = jnp.arange(count)
    between = (index[None, :] > index[:, None]) & (index[None, :] < here)
    reach = jnp.sum(jnp.where(between[:, :, None], logs[None], 0.0), axis=1)
    factor = jnp.where((index < here)[:, None], jnp.exp(reach), 0.0)
    states = everything[:, : state.shape[0]].reshape(count, heads, -1, width)
    return jnp.sum(factor[:, :, None, None] * states.astype(f32), axis=0), columns


def local(
    stream,
    queries,
    keys_in,
    values_in,
    gate_in,
    log_decay,
    head_gain,
    out_weight,
    norm_gain,
    gate_weight,
    up_weight,
    down_weight,
):
    weight_rows, weight_columns = spread_weights(gate_weight, up_weight, down_weight)
    heads = log_decay.shape[1]
    dim = queries.shape[1] // heads
    running, total, within, state = retention(queries, keys_in, values_in, log_decay)
    incoming, weight_columns = incoming_states(total, state, weight_columns)
    mixed = []
    for h in range(heads):
        cut = slice(h * dim, (h + 1) * dim)
        carried = dot(queries[:, cut], incoming[h].astype(bf16))
        retained = within[h] + carried * jnp.exp(running[:, h])[:, None]
        center = jnp.mean(retained, axis=-1, keepdims=True)
        spread = jnp.mean(jnp.square(retained - center), axis=-1, keepdims=True)
        normed = (retained - center) * lax.rsqrt(spread + epsilon) * head_gain[cut].astype(f32)
        mixed.append((jax.nn.silu(gate_in[:, cut].astype(f32)) * normed).astype(bf16))
    terms = dot(jnp.concatenate(mixed, axis=1), out_weight).astype(bf16)
    if lax.axis_size("tp") == 2:
        half = terms.shape[0] // 2
        mine = lax.axis_index("tp") * half
        sent = swap(lax.dynamic_slice_in_dim(terms, half - mine, half, 0), "tp", 1)
        kept = lax.dynamic_slice_in_dim(terms, mine, half, 0)
        attended = kept.astype(f32) + sent.astype(f32)
    else:
        attended = scatter_pair(terms)
    residual = stream.astype(f32) + attended
    normed = (
        residual
        * lax.rsqrt(jnp.mean(residual * residual, axis=-1, keepdims=True) + epsilon)
        * norm_gain.astype(f32)
    ).astype(bf16)

    normed = by_distance(normed)
    normed, weight_rows, weight_columns = lax.optimization_barrier(
        (normed, weight_rows, weight_columns)
    )
    weight_rows = [block for piece in weight_rows for block in near_rest(piece)]
    weight_columns = [
        block for piece in weight_columns for block in near_rest(near_blocks(piece))
    ]
    groups = lax.axis_size("far")
    arrived = [normed] + [swap(normed, "far", s) for s in range(1, groups)]
    rows = [turned(gather_pair(piece), s) for s, piece in enumerate(arrived)]
    gate_full = jnp.concatenate([gate for gate, _ in weight_rows], axis=0)
    up_full = jnp.concatenate([up for _, up in weight_rows], axis=0)
    down_full = jnp.concatenate(
        [jnp.concatenate([part[i] for part in weight_columns], axis=1) for i in range(2)], axis=0
    )
    together = jnp.concatenate(rows, axis=0)
    hidden = (jax.nn.silu(dot(together, gate_full)) * dot(together, up_full)).astype(bf16)
    height = rows[0].shape[0]
    mixer_out = 0.0
    for s in (*range(1, groups), 0):
        part = scatter_pair(dot(hidden[s * height : (s + 1) * height], down_full))
        if s:
            part = turned(swap(part.astype(bf16), "far", s).astype(f32), s)
        mixer_out = mixer_out + part
    return (residual + by_distance(mixer_out)).astype(bf16)


MESH = pl.DeviceIdType.MESH
HIGHEST = lax.Precision.HIGHEST
TAIL = 16
PIECES = 4


def fits(mesh):
    return mesh.shape["tp"] == 2 and mesh.shape["sp"] == GROUP * GROUP


def flip(v, d):
    if d == 0:
        return v
    if d == 1:
        return v + 1 - 2 * lax.rem(v, 2)
    if d == 2:
        return lax.rem(v + 2, 4)
    return 3 - v


def layer_kernel(
    stream_in,
    q_in,
    k_in,
    v_in,
    gate_in,
    decay_in,
    head_gain_in,
    out_weight_in,
    norm_gain_in,
    gate_weight_in,
    up_weight_in,
    down_in,
    result_ref,
    stream_ref,
    q_ref,
    k_ref,
    v_ref,
    gate_ref,
    decay_ref,
    head_gain_ref,
    out_weight_ref,
    norm_gain_ref,
    gate_weight_ref,
    up_weight_ref,
    wide_own,
    wide,
    down,
    rows,
    residual,
    grown,
    within,
    state_out,
    state_in,
    plane_out,
    plane_in,
    carry,
    reach,
    entry_out,
    entry_in,
    mixed,
    term_out,
    term_in,
    hidden,
    part_own,
    part_in,
    sum_own,
    sum_out,
    sum_in,
    in_sem,
    w_send,
    w_relay,
    w_recv,
    w_far,
    st_send,
    st_recv,
    pl_send,
    pl_recv,
    en_send,
    en_recv,
    term_sem,
    row_send,
    row_recv,
    part_sem,
    part_recv,
    sum_send,
    sum_recv,
):
    sp, c = lax.axis_index("sp"), lax.axis_index("tp")
    z, n = lax.div(sp, 4), lax.rem(sp, 4)
    other = 1 - c
    beside = [flip(n, d) for d in range(4)]
    inner = jnp.where(z < 2, 1, -1)
    middle = (z == 1) | (z == 2)
    edge = (z == 0) | (z == 3)
    level = [flip(z, d) for d in (0, 1, 3, 2)]

    def at(zz, nn, cc):
        return (zz * 4 + nn, cc)

    mate = at(z, n, other)

    def copy(src, dst, send, recv, to):
        return pltpu.make_async_remote_copy(
            src_ref=src,
            dst_ref=dst,
            send_sem=send,
            recv_sem=recv,
            device_id=to,
            device_id_type=MESH,
        )

    def arrived(ref, recv):
        copy(ref, ref, recv, recv, mate).wait_recv()

    def left(ref, send):
        copy(ref, ref, send, send, mate).wait_send()

    loads = [
        pltpu.make_async_copy(src, dst, in_sem.at[i])
        for i, (src, dst) in enumerate(
            (
                (decay_in, decay_ref),
                (k_in, k_ref),
                (v_in, v_ref),
                (gate_weight_in, gate_weight_ref),
                (up_weight_in, up_weight_ref),
                (q_in, q_ref),
                (down_in.at[z], down.at[sp]),
                (gate_in, gate_ref),
                (head_gain_in, head_gain_ref),
                (out_weight_in, out_weight_ref),
                (stream_in, stream_ref),
                (norm_gain_in, norm_gain_ref),
            )
        )
    ]
    for load in loads:
        load.start()

    barrier = pltpu.get_barrier_semaphore()
    partners = [mate]
    partners += [at(z, beside[d], c) for d in (1, 2, 3)]
    partners += [at(flip(z, d), n, c) for d in (1, 2, 3)]
    for to in partners:
        pl.semaphore_signal(barrier, inc=1, device_id=to, device_id_type=MESH)

    units = down.shape[1]
    heads = decay_ref.shape[0]
    dim = q_ref.shape[1] // heads
    count = q_ref.shape[0]
    scale = dim ** (-0.5)
    loads[0].wait()
    decay = decay_ref[...]
    low = lax.broadcasted_iota(jnp.int32, (count, count), 0)
    high = lax.broadcasted_iota(jnp.int32, (count, count), 1)
    causal = low >= high
    running = jnp.dot(
        decay, (low <= high).astype(f32), precision=HIGHEST, preferred_element_type=f32
    )
    line = lax.broadcasted_iota(jnp.int32, (TAIL, dim), 0)
    loads[1].wait()
    loads[2].wait()
    cols = []
    for h in range(heads):
        side = slice(h * dim, (h + 1) * dim)
        col = jnp.broadcast_to(running[h : h + 1], (dim, count)).T
        cols.append(col)
        total = running[h : h + 1, count - 1 : count]
        tail = jnp.exp(total - col) * scale
        keyed = (k_ref[:, side].astype(f32) * tail).T.astype(bf16)
        state = jnp.dot(keyed, v_ref[:, side], preferred_element_type=f32)
        state_out[h, :dim] = state.astype(bf16)
        state_out[h, dim:] = split_total(total, line)

    loads[3].wait()
    loads[4].wait()
    for g in range(wide_own.shape[0]):
        side = slice(g * units, (g + 1) * units)
        wide_own[g] = jnp.concatenate(
            [gate_weight_ref[:, side], up_weight_ref[:, side]], axis=1
        )
    pl.semaphore_wait(barrier, len(partners))

    full = (wide, down)
    given = (wide_own, down_in)
    cut = (wide.shape[1] // 2, down.shape[1] // 2)

    def far(d, kind, part=None):
        half = cut[kind]
        some = pl.ds(0, 2 * half) if part is None else pl.ds(part * half, half)
        copy(
            given[kind].at[level[d], some],
            full[kind].at[sp, some],
            w_far.at[kind, d - 1],
            w_recv.at[kind, sp, 0],
            at(level[d], n, c),
        ).start()

    def push(d, kind):
        slot = level[d] * 4 + n
        if d:
            arrived(full[kind].at[slot], w_recv.at[kind, slot, 0])
        src = full[kind].at[slot] if d else given[kind].at[z]
        for a in (1, 2):
            copy(
                src,
                full[kind].at[slot],
                w_send.at[kind, d, a - 1],
                w_recv.at[kind, slot, 0],
                at(z, beside[a], c),
            ).start()

    def relay(d, kind):
        half = cut[kind]
        for a in (1, 2):
            slot = level[d] * 4 + beside[a]
            arrived(full[kind].at[slot], w_recv.at[kind, slot, 0])
            part = pl.ds(0, half) if a == 1 else pl.ds(half, half)
            piece = full[kind].at[slot, part]
            copy(
                piece,
                piece,
                w_relay.at[kind, d, a - 1],
                w_recv.at[kind, slot, a - 1],
                at(z, beside[3 - a], c),
            ).start()

    def finish(d, kind):
        half = cut[kind]
        slot = level[d] * 4 + beside[3]
        arrived(full[kind].at[slot, pl.ds(0, half)], w_recv.at[kind, slot, 0])
        arrived(full[kind].at[slot, pl.ds(half, half)], w_recv.at[kind, slot, 1])

    def settle_weights():
        for kind in (0, 1):
            half = cut[kind]
            for d in range(4):
                if d:
                    left(given[kind].at[0], w_far.at[kind, d - 1])
                for a in (0, 1):
                    left(given[kind].at[0], w_send.at[kind, d, a])
                    left(full[kind].at[0, pl.ds(0, half)], w_relay.at[kind, d, a])

    for d in (1, 2, 3):
        copy(
            state_out.at[beside[d]],
            state_in.at[n],
            st_send.at[d - 1],
            st_recv.at[d - 1],
            at(z, beside[d], c),
        ).start()
    state_in[n] = state_out[n]
    push(0, 0)
    far(1, 0, 0)

    @pl.when(z == 1)
    def _():
        far(2, 0, 0)

    @pl.when(z == 2)
    def _():
        far(2, 0)

    wide[sp] = wide_own[z]

    for d in (1, 2, 3):
        arrived(state_in.at[beside[d]], st_recv.at[d - 1])
    totals = [join_total(state_in[m, dim:]) for m in range(4)]
    states = [state_in[m, :dim].astype(f32) for m in range(4)]
    plane, span = states[0], totals[0]
    for m in range(1, 4):
        plane = plane * jnp.exp(totals[m]) + states[m]
        span = span + totals[m]
    plane_out[:dim] = plane.astype(bf16)
    plane_out[dim:] = split_total(span, line)
    for k in (1, 2, 3):

        @pl.when(z + k <= 3)
        def _():
            copy(
                plane_out,
                plane_in.at[z],
                pl_send.at[k - 1],
                pl_recv.at[z],
                at(z + k, n, c),
            ).start()

    far(1, 0, 1)

    @pl.when(edge)
    def _():
        far(2, 0)

    @pl.when(z == 1)
    def _():
        far(2, 0, 1)

    far(3, 0)

    loads[5].wait()
    for h in range(heads):
        side = slice(h * dim, (h + 1) * dim)
        q, k, v = q_ref[:, side], k_ref[:, side], v_ref[:, side]
        gap = jnp.minimum(cols[h][:, :1] - running[h : h + 1], 0.0)
        table = jnp.where(causal, jnp.exp(gap), 0.0) * scale
        scores = dot(q, k, ((1,), (1,)))
        within[:, side] = jnp.dot(
            (scores * table).astype(bf16), v, preferred_element_type=f32
        )
        grown[h] = jnp.exp(cols[h])

    carry[...] = jnp.zeros_like(carry)
    reach[...] = jnp.zeros_like(reach)
    for k in (1, 2, 3):

        @pl.when(z >= k)
        def _():
            arrived(plane_in.at[z - k], pl_recv.at[z - k])
            carry[...] += jnp.exp(reach[...]) * plane_in[z - k, :dim].astype(f32)
            reach[...] += join_total(plane_in[z - k, dim:])

    entry = carry[...]
    for m in range(4):
        entry_out[m] = entry.astype(bf16)
        if m < 3:
            entry = entry * jnp.exp(totals[m]) + states[m]
    for d in (1, 2, 3):
        copy(
            entry_out.at[beside[d]],
            entry_in.at[n],
            en_send.at[d - 1],
            en_recv.at[d - 1],
            at(z, beside[d], c),
        ).start()
    entry_in[n] = entry_out[n]

    relay(0, 0)
    push(1, 0)

    for d in (1, 2, 3):
        arrived(entry_in.at[beside[d]], en_recv.at[d - 1])
    for load in loads[6:]:
        load.wait()
    for h in range(heads):
        side = slice(h * dim, (h + 1) * dim)
        carried = jnp.dot(q_ref[:, side], entry_in[h], preferred_element_type=f32)
        retained = within[:, side] + carried * grown[h]
        center = jnp.mean(retained, axis=-1, keepdims=True)
        away = retained - center
        spread = jnp.mean(away * away, axis=-1, keepdims=True)
        normed = away * lax.rsqrt(spread + epsilon) * head_gain_ref[side][None].astype(f32)
        gate = gate_ref[:, side].astype(f32)
        mixed[:, side] = (jax.nn.silu(gate) * normed).astype(bf16)

    half = count // 2
    give = pl.ds(pl.multiple_of(other * half, half), half)
    keep = pl.ds(pl.multiple_of(c * half, half), half)
    term_out[...] = jnp.dot(
        mixed[give], out_weight_ref[...], preferred_element_type=f32
    ).astype(bf16)
    copy(term_out, term_in, term_sem.at[0], term_sem.at[1], mate).start()
    kept = jnp.dot(mixed[keep], out_weight_ref[...], preferred_element_type=f32)
    residual[...] = stream_ref[...].astype(f32) + kept.astype(bf16).astype(f32)
    arrived(term_in, term_sem.at[1])
    total = residual[...] + term_in[...].astype(f32)
    residual[...] = total
    mean = jnp.mean(total * total, axis=-1, keepdims=True)
    rows[z, c] = (
        total * lax.rsqrt(mean + epsilon) * norm_gain_ref[...][None].astype(f32)
    ).astype(bf16)

    pieces = PIECES
    high = half // pieces

    def strip(p):
        return pl.ds(p * high, high)

    def pass_on(zz, way, p):
        piece = rows.at[zz, c, strip(p)]
        copy(
            piece,
            piece,
            row_send.at[way, zz, p],
            row_recv.at[min(way, 1), zz, p],
            (mate, at(z + inner, n, c), at(z - inner, n, c))[way],
        ).start()

    def from_outer():
        @pl.when(middle)
        def _():
            zz = z - inner
            for p in range(pieces):
                arrived(rows.at[zz, c, strip(p)], row_recv.at[1, zz, p])
                pass_on(zz, 1, p)
                pass_on(zz, 0, p)

    def from_inner(k, *parts):
        def go():
            zz = z + inner * k
            for p in parts:
                arrived(rows.at[zz, c, strip(p)], row_recv.at[1, zz, p])
                if k < 3:

                    @pl.when(middle)
                    def _():
                        pass_on(zz, 2, p)

                pass_on(zz, 0, p)

        if k < 3:
            go()
        else:
            pl.when(edge)(go)

    for p in range(pieces):
        pass_on(z, 1, p)

        @pl.when(middle)
        def _():
            pass_on(z, 2, p)

        pass_on(z, 0, p)

    relay(1, 0)
    push(2, 0)
    relay(2, 0)
    push(3, 0)
    from_outer()

    @pl.when(edge)
    def _():
        far(1, 1)

    from_inner(1, 0, 1, 2, 3)
    relay(3, 0)
    push(0, 1)
    from_inner(2, 0, 1)
    for d in range(4):
        finish(d, 0)

    depth = rows.shape[3]

    def raise_rows(j):
        zt = z + inner * jnp.where(edge, j, (0, -1, 1, 2)[j])
        for p in range(pieces):
            arrived(rows.at[zt, other, strip(p)], row_recv.at[0, zt, p])
        both = jnp.dot(
            rows[zt].reshape(count, depth),
            wide[...].reshape(depth, 2 * units),
            preferred_element_type=f32,
        )
        hidden[zt] = (jax.nn.silu(both[:, :units]) * both[:, units:]).astype(bf16)

    raise_rows(0)
    from_inner(2, 2)
    raise_rows(1)
    relay(0, 1)
    from_inner(2, 3)

    raise_rows(2)
    from_inner(3, 0, 1, 2, 3)
    raise_rows(3)

    @pl.when(middle)
    def _():
        far(1, 1)

    far(2, 1)
    far(3, 1)

    def turn(j):
        return z + inner * jnp.where(
            edge, 3 - j, jnp.where(j == 2, -1, jnp.where(j == 3, 0, j + 1))
        )

    def send_sum(zt, p, to, side):
        copy(
            sum_out.at[zt, p],
            sum_in.at[side, zt, p],
            sum_send.at[zt, p],
            sum_recv.at[side, zt, p],
            to,
        ).start()

    def lower(q):
        p = level[q]
        weight = jnp.concatenate([down[p * 4 + m] for m in range(4)], axis=1)

        def product(j, carried):
            zt = turn(j)
            out = jnp.dot(hidden[zt], weight, preferred_element_type=f32).astype(bf16)
            part_own[zt, p, 0] = out[:half]
            part_own[zt, p, 1] = out[half:]
            copy(
                part_own.at[zt, p, other],
                part_in.at[zt, p],
                part_sem.at[zt, p],
                part_recv.at[zt, p],
                mate,
            ).start()
            return carried

        def gather(j, carried):
            zt = turn(j)
            arrived(part_in.at[zt, p], part_recv.at[zt, p])
            both = part_own[zt, p, c].astype(f32) + part_in[zt, p].astype(f32)
            sum_own[zt, p] = both

            @pl.when(edge & (zt != z))
            def _():
                sum_out[zt, p] = both.astype(bf16)

            @pl.when(edge & (j < (3 if q < 2 else 2)))
            def _():
                send_sum(zt, p, at(z + inner, n, c), 0)

            return carried

        lax.fori_loop(0, GROUP, product, 0)
        lax.fori_loop(0, GROUP, gather, 0)

    def add_on(zt, p, side, to):
        arrived(sum_in.at[side, zt, p], sum_recv.at[side, zt, p])
        sum_out[zt, p] = (sum_own[zt, p] + sum_in[side, zt, p].astype(f32)).astype(bf16)
        send_sum(zt, p, to, 1)

    def inward(i):
        p = flip(z - inner, (0, 1, 3, 2)[i])
        add_on(z + 2 * inner, p, 0, at(z + inner, n, c))
        add_on(z + inner, p, 0, at(z + inner, n, c))

    def outward(i):
        p = flip(z + 2 * inner, (0, 1, 3, 2)[i])
        add_on(z - inner, p, 1, at(z - inner, n, c))

    finish(0, 1)
    lower(0)
    push(1, 1)
    relay(1, 1)
    push(2, 1)
    push(3, 1)
    finish(1, 1)
    lower(1)

    @pl.when(middle)
    def _():
        inward(0)

    relay(2, 1)
    relay(3, 1)
    finish(2, 1)
    lower(2)
    finish(3, 1)
    lower(3)

    @pl.when(edge)
    def _():
        for q in (2, 3):
            send_sum(z + inner, level[q], at(z + inner, n, c), 0)

    @pl.when(middle)
    def _():
        inward(1)
        outward(0)
        outward(1)
        inward(2)
        outward(2)
        inward(3)
        outward(3)

    wide_step = depth // GROUP
    for p in range(GROUP):
        side = slice(p * wide_step, (p + 1) * wide_step)
        residual[:, side] += sum_own[z, p]

        @pl.when(middle)
        def _():
            arrived(sum_in.at[0, z, p], sum_recv.at[0, z, p])
            residual[:, side] += sum_in[0, z, p].astype(f32)

    for p in range(GROUP):
        side = slice(p * wide_step, (p + 1) * wide_step)
        arrived(sum_in.at[1, z, p], sum_recv.at[1, z, p])
        result_ref[:, side] = (
            residual[:, side] + sum_in[1, z, p].astype(f32)
        ).astype(result_ref.dtype)

    settle_weights()
    for d in (1, 2, 3):
        left(state_out.at[0], st_send.at[d - 1])
        left(entry_out.at[0], en_send.at[d - 1])
        for p in range(GROUP):
            left(sum_out.at[0, 0], sum_send.at[flip(z, d), p])

        @pl.when(z + d <= 3)
        def _():
            left(plane_out, pl_send.at[d - 1])

    left(term_out, term_sem.at[0])
    for zz in range(GROUP):
        for p in range(GROUP):
            left(part_in.at[0, 0], part_sem.at[zz, p])
        for p in range(pieces):
            left(rows.at[0, 0, strip(0)], row_send.at[0, zz, p])
    for p in range(pieces):
        left(rows.at[0, 0, strip(0)], row_send.at[1, z, p])

        @pl.when(middle)
        def _():
            left(rows.at[0, 0, strip(0)], row_send.at[1, z - inner, p])
            for k in range(3):
                left(rows.at[0, 0, strip(0)], row_send.at[2, z + inner * k, p])


def split_total(total, line):
    top = total.astype(bf16).astype(f32)
    mid = (total - top).astype(bf16).astype(f32)
    low = total - top - mid
    return jnp.where(line == 0, top, jnp.where(line == 1, mid, low)).astype(bf16)


def join_total(parts):
    parts = parts.astype(f32)
    return parts[0:1] + parts[1:2] + parts[2:3]


def fused_local(
    stream,
    queries,
    keys_in,
    values_in,
    gate_in,
    log_decay,
    head_gain,
    out_weight,
    norm_gain,
    gate_weight,
    up_weight,
    down_weight,
):
    count, heads = log_decay.shape
    width = queries.shape[1]
    dim = width // heads
    depth = stream.shape[1]
    own, units = gate_weight.shape
    sizes = GROUP * GROUP
    part = units // GROUP
    down = down_weight.reshape(GROUP, part, down_weight.shape[1])
    half = count // 2
    vmem = pltpu.VMEM
    dma = pltpu.SemaphoreType.DMA
    given = (
        stream,
        queries,
        keys_in,
        values_in,
        gate_in,
        log_decay.T,
        head_gain,
        out_weight,
        norm_gain,
        gate_weight,
        up_weight,
    )
    return pl.pallas_call(
        layer_kernel,
        out_shape=jax.ShapeDtypeStruct((half, depth), bf16),
        in_specs=[pl.BlockSpec(memory_space=pl.ANY)] * 12,
        out_specs=pl.BlockSpec(memory_space=vmem),
        scratch_shapes=[
            *(vmem(value.shape, value.dtype) for value in given),
            vmem((GROUP, own, 2 * part), bf16),
            vmem((sizes, own, 2 * part), bf16),
            vmem((sizes, part, down_weight.shape[1]), bf16),
            vmem((GROUP, 2, half, depth), bf16),
            vmem((half, depth), f32),
            vmem((heads, count, dim), f32),
            vmem((count, width), f32),
            vmem((heads, dim + TAIL, dim), bf16),
            vmem((heads, dim + TAIL, dim), bf16),
            vmem((dim + TAIL, dim), bf16),
            vmem((GROUP, dim + TAIL, dim), bf16),
            vmem((dim, dim), f32),
            vmem((1, dim), f32),
            vmem((heads, dim, dim), bf16),
            vmem((heads, dim, dim), bf16),
            vmem((count, width), bf16),
            vmem((half, depth), bf16),
            vmem((half, depth), bf16),
            vmem((GROUP, count, part), bf16),
            vmem((GROUP, GROUP, 2, half, depth // GROUP), bf16),
            vmem((GROUP, GROUP, half, depth // GROUP), bf16),
            vmem((GROUP, GROUP, half, depth // GROUP), f32),
            vmem((GROUP, GROUP, half, depth // GROUP), bf16),
            vmem((2, GROUP, GROUP, half, depth // GROUP), bf16),
            dma((12,)),
            dma((2, GROUP, 2)),
            dma((2, GROUP, 2)),
            dma((2, sizes, 2)),
            dma((2, GROUP - 1)),
            dma((3,)),
            dma((3,)),
            dma((3,)),
            dma((GROUP,)),
            dma((3,)),
            dma((3,)),
            dma((2,)),
            dma((3, GROUP, PIECES)),
            dma((2, GROUP, PIECES)),
            dma((GROUP, GROUP)),
            dma((GROUP, GROUP)),
            dma((GROUP, GROUP)),
            dma((2, GROUP, GROUP)),
        ],
        compiler_params=pltpu.CompilerParams(
            collective_id=0, has_side_effects=True, vmem_limit_bytes=60 * 1024 * 1024
        ),
        name="layer",
    )(*given, down)


def fused(mesh):
    return jax.shard_map(
        fused_local,
        mesh=mesh,
        in_specs=(
            P(("sp", "tp"), None),
            P("sp", "tp"),
            P("sp", "tp"),
            P("sp", "tp"),
            P("sp", "tp"),
            P("sp", "tp"),
            P("tp"),
            P("tp", None),
            P(),
            P("sp", "tp"),
            P("sp", "tp"),
            P("tp", "sp"),
        ),
        out_specs=P(("sp", "tp"), None),
        check_vma=False,
    )


def solution(mesh):
    if fits(mesh):
        return fused(mesh)
    devices = mesh.devices
    count, pair = devices.shape
    split = Mesh(devices.reshape(GROUP, count // GROUP, pair), (*SP, "tp"))
    return jax.shard_map(
        local,
        mesh=split,
        in_specs=(
            P((*SP, "tp"), None),
            P(SP, "tp"),
            P(SP, "tp"),
            P(SP, "tp"),
            P(SP, "tp"),
            P(SP, "tp"),
            P("tp"),
            P("tp", None),
            P(),
            P(SP, "tp"),
            P(SP, "tp"),
            P("tp", SP),
        ),
        out_specs=P((*SP, "tp"), None),
        check_vma=False,
    )
```

```python
import functools

import jax
import jax.numpy as jnp
from jax import lax
from jax.experimental import pallas as pl
from jax.experimental.pallas import tpu as pltpu
from jax.sharding import Mesh, PartitionSpec as P

epsilon = 1e-06
GROUP = 4
SP = ("far", "near")
f32, bf16 = jnp.float32, jnp.bfloat16


def swap(value, axis, bits):
    size = lax.axis_size(axis)
    return lax.ppermute(value, axis, [(i, i ^ bits) for i in range(size)])


def near_blocks(value):
    size = lax.axis_size("near")
    steps = (1, 2) if size == 4 else range(1, size)
    return [value] + [swap(value, "near", s) for s in steps]


def near_rest(blocks):
    half = blocks[0].shape[0] // 2
    cut = [(block[:half], block[half:]) for block in blocks]
    if lax.axis_size("near") == 4:
        cut.append((swap(cut[1][0], "near", 2), swap(cut[2][1], "near", 1)))
    return cut


def spread_weights(gate_weight, up_weight, down_weight):
    groups = lax.axis_size("far")
    far_at = lax.axis_index("far")
    width = gate_weight.shape[1] // groups
    all_rows, all_columns = [], []
    for s in range(groups):
        at = (far_at ^ s) * width
        rows = jnp.concatenate(
            [
                lax.dynamic_slice_in_dim(gate_weight, at, width, 1),
                lax.dynamic_slice_in_dim(up_weight, at, width, 1),
            ],
            axis=0,
        )
        all_rows.append(swap(rows, "far", s) if s else rows)
    for s in range(groups):
        at = (far_at ^ s) * width
        all_columns.append(lax.dynamic_slice_in_dim(down_weight, at, width, 0))
    return [near_blocks(piece) for piece in all_rows], all_columns


def by_distance(value):
    groups, near = lax.axis_size("far"), lax.axis_size("near")
    here = lax.axis_index("far") * near + lax.axis_index("near")
    width = value.shape[1] // (groups * near)
    return jnp.concatenate(
        [
            lax.dynamic_slice_in_dim(value, (here ^ k) * width, width, 1)
            for k in range(groups * near)
        ],
        axis=1,
    )


def turned(value, bits):
    groups = lax.axis_size("far")
    width = value.shape[1] // groups
    return jnp.concatenate(
        [value[:, (g ^ bits) * width : ((g ^ bits) + 1) * width] for g in range(groups)], axis=1
    )


def gather_pair(rows):
    if lax.axis_size("tp") == 2:
        return jnp.concatenate([rows, swap(rows, "tp", 1)], axis=0)
    return lax.all_gather(rows, "tp", axis=0, tiled=True)


def scatter_pair(terms):
    terms = terms.astype(bf16)
    if lax.axis_size("tp") == 2:
        half = terms.shape[0] // 2
        return terms[:half].astype(f32) + swap(terms[half:], "tp", 1).astype(f32)
    return lax.psum_scatter(terms, "tp", scatter_dimension=0, tiled=True).astype(f32)


def dot(a, b, dims=((1,), (0,))):
    return lax.dot_general(a, b, (dims, ((), ())), preferred_element_type=f32)


def retention(queries, keys_in, values_in, log_decay):
    row_count, heads = log_decay.shape
    dim = queries.shape[1] // heads
    scale = dim ** (-0.5)
    running = jnp.cumsum(log_decay, axis=0)
    total = running[-1]
    offsets = jnp.arange(row_count)
    causal = offsets[:, None] >= offsets[None, :]
    within, states = [], []
    for h in range(heads):
        cut = slice(h * dim, (h + 1) * dim)
        q, k, v = queries[:, cut], keys_in[:, cut], values_in[:, cut]
        col = running[:, h]
        gap = jnp.minimum(col[:, None] - col[None, :], 0.0)
        table = jnp.where(causal, jnp.exp(gap), 0.0) * scale
        within.append(dot((dot(q, k, ((1,), (1,))) * table).astype(bf16), v))
        tail = (jnp.exp(total[h] - col) * scale)[:, None]
        states.append(dot((k.astype(f32) * tail).astype(bf16), v, ((0,), (0,))))
    return running, total, within, jnp.concatenate(states, axis=0)


def incoming_states(total, state, columns):
    heads = total.shape[0]
    near = lax.axis_size("near")
    here = lax.axis_index("far") * near + lax.axis_index("near")
    high = lax.reduce_precision(total, 8, 7)
    mid = lax.reduce_precision(total - high, 8, 7)
    low = total - high - mid
    parts = jnp.concatenate([high, mid, low])
    extra = -(-parts.shape[0] // 16) * 16
    parts = jnp.pad(parts, (0, extra - parts.shape[0]))
    width = state.shape[1]
    packed = jnp.concatenate(
        [state.astype(bf16), jnp.broadcast_to(parts[:, None], (extra, width)).astype(bf16)], axis=0
    )
    everything = lax.all_gather(packed, SP)
    everything, columns = lax.optimization_barrier((everything, columns))
    columns = [swap(piece, "far", s) if s else piece for s, piece in enumerate(columns)]
    count = everything.shape[0]
    logs = everything[:, state.shape[0] : state.shape[0] + 3 * heads, 0].astype(f32)
    logs = logs.reshape(count, 3, heads).sum(axis=1)
    index = jnp.arange(count)
    between = (index[None, :] > index[:, None]) & (index[None, :] < here)
    reach = jnp.sum(jnp.where(between[:, :, None], logs[None], 0.0), axis=1)
    factor = jnp.where((index < here)[:, None], jnp.exp(reach), 0.0)
    states = everything[:, : state.shape[0]].reshape(count, heads, -1, width)
    return jnp.sum(factor[:, :, None, None] * states.astype(f32), axis=0), columns


def local(
    stream,
    queries,
    keys_in,
    values_in,
    gate_in,
    log_decay,
    head_gain,
    out_weight,
    norm_gain,
    gate_weight,
    up_weight,
    down_weight,
):
    weight_rows, weight_columns = spread_weights(gate_weight, up_weight, down_weight)
    heads = log_decay.shape[1]
    dim = queries.shape[1] // heads
    running, total, within, state = retention(queries, keys_in, values_in, log_decay)
    incoming, weight_columns = incoming_states(total, state, weight_columns)
    mixed = []
    for h in range(heads):
        cut = slice(h * dim, (h + 1) * dim)
        carried = dot(queries[:, cut], incoming[h].astype(bf16))
        retained = within[h] + carried * jnp.exp(running[:, h])[:, None]
        center = jnp.mean(retained, axis=-1, keepdims=True)
        spread = jnp.mean(jnp.square(retained - center), axis=-1, keepdims=True)
        normed = (retained - center) * lax.rsqrt(spread + epsilon) * head_gain[cut].astype(f32)
        mixed.append((jax.nn.silu(gate_in[:, cut].astype(f32)) * normed).astype(bf16))
    terms = dot(jnp.concatenate(mixed, axis=1), out_weight).astype(bf16)
    if lax.axis_size("tp") == 2:
        half = terms.shape[0] // 2
        mine = lax.axis_index("tp") * half
        sent = swap(lax.dynamic_slice_in_dim(terms, half - mine, half, 0), "tp", 1)
        kept = lax.dynamic_slice_in_dim(terms, mine, half, 0)
        attended = kept.astype(f32) + sent.astype(f32)
    else:
        attended = scatter_pair(terms)
    residual = stream.astype(f32) + attended
    normed = (
        residual
        * lax.rsqrt(jnp.mean(residual * residual, axis=-1, keepdims=True) + epsilon)
        * norm_gain.astype(f32)
    ).astype(bf16)

    normed = by_distance(normed)
    normed, weight_rows, weight_columns = lax.optimization_barrier(
        (normed, weight_rows, weight_columns)
    )
    weight_rows = [block for piece in weight_rows for block in near_rest(piece)]
    weight_columns = [
        block for piece in weight_columns for block in near_rest(near_blocks(piece))
    ]
    groups = lax.axis_size("far")
    arrived = [normed] + [swap(normed, "far", s) for s in range(1, groups)]
    rows = [turned(gather_pair(piece), s) for s, piece in enumerate(arrived)]
    gate_full = jnp.concatenate([gate for gate, _ in weight_rows], axis=0)
    up_full = jnp.concatenate([up for _, up in weight_rows], axis=0)
    down_full = jnp.concatenate(
        [jnp.concatenate([part[i] for part in weight_columns], axis=1) for i in range(2)], axis=0
    )
    together = jnp.concatenate(rows, axis=0)
    hidden = (jax.nn.silu(dot(together, gate_full)) * dot(together, up_full)).astype(bf16)
    height = rows[0].shape[0]
    mixer_out = 0.0
    for s in (*range(1, groups), 0):
        part = scatter_pair(dot(hidden[s * height : (s + 1) * height], down_full))
        if s:
            part = turned(swap(part.astype(bf16), "far", s).astype(f32), s)
        mixer_out = mixer_out + part
    return (residual + by_distance(mixer_out)).astype(bf16)


MESH = pl.DeviceIdType.MESH
HIGHEST = lax.Precision.HIGHEST
TAIL = 16
PIECES = 4


def fits(mesh):
    return mesh.shape["tp"] == 2 and mesh.shape["sp"] == GROUP * GROUP


def flip(v, d):
    if d == 0:
        return v
    if d == 1:
        return v + 1 - 2 * lax.rem(v, 2)
    if d == 2:
        return lax.rem(v + 2, 4)
    return 3 - v


def layer_kernel(
    stream_in,
    q_in,
    k_in,
    v_in,
    gate_in,
    decay_in,
    head_gain_in,
    out_weight_in,
    norm_gain_in,
    gate_weight_in,
    up_weight_in,
    down_in,
    result_ref,
    stream_ref,
    q_ref,
    k_ref,
    v_ref,
    gate_ref,
    decay_ref,
    head_gain_ref,
    out_weight_ref,
    norm_gain_ref,
    gate_weight_ref,
    up_weight_ref,
    wide_own,
    wide,
    down,
    transit,
    rows,
    residual,
    grown,
    within,
    state_out,
    state_in,
    plane_out,
    plane_in,
    carry,
    reach,
    entry_out,
    entry_in,
    mixed,
    term_out,
    term_in,
    hidden,
    part_own,
    part_in,
    sum_own,
    sum_out,
    sum_in,
    result,
    in_sem,
    out_sem,
    w_send,
    w_relay,
    w_recv,
    w_far,
    transit_send,
    transit_recv,
    st_send,
    st_recv,
    pl_send,
    pl_recv,
    en_send,
    en_recv,
    term_sem,
    row_send,
    row_recv,
    part_sem,
    part_recv,
    sum_send,
    sum_recv,
):
    sp, c = lax.axis_index("sp"), lax.axis_index("tp")
    z, n = lax.div(sp, 4), lax.rem(sp, 4)
    other = 1 - c
    beside = [flip(n, d) for d in range(4)]
    inner = jnp.where(z < 2, 1, -1)
    middle = (z == 1) | (z == 2)
    edge = (z == 0) | (z == 3)
    ends = [jnp.where(edge, flip(z, d), flip(z, 5 - d)) for d in (2, 3)]
    level = (
        [flip(z, d) for d in (0, 1, 3, 2)],
        [z, flip(z, 1), *ends],
    )

    def at(zz, nn, cc):
        return (zz * 4 + nn, cc)

    mate = at(z, n, other)

    def copy(src, dst, send, recv, to):
        return pltpu.make_async_remote_copy(
            src_ref=src,
            dst_ref=dst,
            send_sem=send,
            recv_sem=recv,
            device_id=to,
            device_id_type=MESH,
        )

    def arrived(ref, recv):
        copy(ref, ref, recv, recv, mate).wait_recv()

    def left(ref, send):
        copy(ref, ref, send, send, mate).wait_send()

    loads = [
        pltpu.make_async_copy(src, dst, in_sem.at[i])
        for i, (src, dst) in enumerate(
            (
                (decay_in, decay_ref),
                (k_in, k_ref),
                (v_in, v_ref),
                (gate_weight_in, gate_weight_ref),
                (up_weight_in, up_weight_ref),
                (q_in, q_ref),
                (down_in.at[z], down.at[sp]),
                (gate_in, gate_ref),
                (head_gain_in, head_gain_ref),
                (out_weight_in, out_weight_ref),
                (stream_in, stream_ref),
                (norm_gain_in, norm_gain_ref),
            )
        )
    ]
    for load in loads:
        load.start()

    barrier = pltpu.get_barrier_semaphore()
    partners = [mate]
    partners += [at(z, beside[d], c) for d in (1, 2, 3)]
    partners += [at(flip(z, d), n, c) for d in (1, 2, 3)]
    for to in partners:
        pl.semaphore_signal(barrier, inc=1, device_id=to, device_id_type=MESH)

    units = down.shape[1]
    heads = decay_ref.shape[0]
    dim = q_ref.shape[1] // heads
    count = q_ref.shape[0]
    scale = dim ** (-0.5)
    loads[0].wait()
    decay = decay_ref[...]
    low = lax.broadcasted_iota(jnp.int32, (count, count), 0)
    high = lax.broadcasted_iota(jnp.int32, (count, count), 1)
    causal = low >= high
    running = jnp.dot(
        decay, (low <= high).astype(f32), precision=HIGHEST, preferred_element_type=f32
    )
    line = lax.broadcasted_iota(jnp.int32, (TAIL, dim), 0)
    loads[1].wait()
    loads[2].wait()
    cols = []
    for h in range(heads):
        side = slice(h * dim, (h + 1) * dim)
        col = jnp.broadcast_to(running[h : h + 1], (dim, count)).T
        cols.append(col)
        total = running[h : h + 1, count - 1 : count]
        tail = jnp.exp(total - col) * scale
        keyed = (k_ref[:, side].astype(f32) * tail).T.astype(bf16)
        state = jnp.dot(keyed, v_ref[:, side], preferred_element_type=f32)
        state_out[h, :dim] = state.astype(bf16)
        state_out[h, dim:] = split_total(total, line)

    loads[3].wait()
    loads[4].wait()
    for g in range(wide_own.shape[0]):
        side = slice(g * units, (g + 1) * units)
        wide_own[g] = jnp.concatenate(
            [gate_weight_ref[:, side], up_weight_ref[:, side]], axis=1
        )
    pl.semaphore_wait(barrier, len(partners))

    full = (wide, down)
    given = (wide_own, down_in)
    cut = (wide.shape[1] // 2, down.shape[1] // 2)

    def far(d, kind, part=None):
        half = cut[kind]
        some = pl.ds(0, 2 * half) if part is None else pl.ds(part * half, half)
        copy(
            given[kind].at[level[kind][d], some],
            full[kind].at[sp, some],
            w_far.at[kind, d - 1],
            w_recv.at[kind, sp, 0],
            at(level[kind][d], n, c),
        ).start()

    def early(k):
        copy(
            down_in.at[z + inner * (k + 2)],
            transit.at[k],
            w_far.at[1, k + 1],
            transit_recv.at[k],
            at(z + inner, n, c),
        ).start()

    def onward(k):
        arrived(transit.at[k], transit_recv.at[k])
        slot = (z - inner) * 4 + n
        copy(
            transit.at[k],
            down.at[slot],
            transit_send.at[k],
            w_recv.at[1, slot, 0],
            at(z + inner * (k + 1), n, c),
        ).start()

    def push(d, kind):
        slot = level[kind][d] * 4 + n
        if d:
            arrived(full[kind].at[slot], w_recv.at[kind, slot, 0])
        src = full[kind].at[slot] if d else given[kind].at[z]
        for a in (1, 2):
            copy(
                src,
                full[kind].at[slot],
                w_send.at[kind, d, a - 1],
                w_recv.at[kind, slot, 0],
                at(z, beside[a], c),
            ).start()

    def relay(d, kind):
        half = cut[kind]
        for a in (1, 2):
            slot = level[kind][d] * 4 + beside[a]
            arrived(full[kind].at[slot], w_recv.at[kind, slot, 0])
            part = pl.ds(0, half) if a == 1 else pl.ds(half, half)
            piece = full[kind].at[slot, part]
            copy(
                piece,
                piece,
                w_relay.at[kind, d, a - 1],
                w_recv.at[kind, slot, a - 1],
                at(z, beside[3 - a], c),
            ).start()

    def finish(d, kind):
        half = cut[kind]
        slot = level[kind][d] * 4 + beside[3]
        arrived(full[kind].at[slot, pl.ds(0, half)], w_recv.at[kind, slot, 0])
        arrived(full[kind].at[slot, pl.ds(half, half)], w_recv.at[kind, slot, 1])

    def settle_weights():
        for kind in (0, 1):
            half = cut[kind]
            for d in range(4):
                if (kind, d) == (1, 1):

                    @pl.when(edge)
                    def _():
                        left(given[kind].at[0], w_far.at[kind, d - 1])

                elif d:
                    left(given[kind].at[0], w_far.at[kind, d - 1])
                for a in (0, 1):
                    left(given[kind].at[0], w_send.at[kind, d, a])
                    left(full[kind].at[0, pl.ds(0, half)], w_relay.at[kind, d, a])

    for d in (1, 2, 3):
        copy(
            state_out.at[beside[d]],
            state_in.at[n],
            st_send.at[d - 1],
            st_recv.at[d - 1],
            at(z, beside[d], c),
        ).start()
    state_in[n] = state_out[n]
    push(0, 0)
    far(1, 0, 0)

    @pl.when(z == 1)
    def _():
        far(2, 0, 0)

    @pl.when(z == 2)
    def _():
        far(2, 0)

    wide[sp] = wide_own[z]

    for d in (1, 2, 3):
        arrived(state_in.at[beside[d]], st_recv.at[d - 1])
    totals = [join_total(state_in[m, dim:]) for m in range(4)]
    states = [state_in[m, :dim].astype(f32) for m in range(4)]
    plane, span = states[0], totals[0]
    for m in range(1, 4):
        plane = plane * jnp.exp(totals[m]) + states[m]
        span = span + totals[m]
    plane_out[:dim] = plane.astype(bf16)
    plane_out[dim:] = split_total(span, line)
    for k in (1, 2, 3):

        @pl.when(z + k <= 3)
        def _():
            copy(
                plane_out,
                plane_in.at[z],
                pl_send.at[k - 1],
                pl_recv.at[z],
                at(z + k, n, c),
            ).start()

    far(1, 0, 1)

    @pl.when(edge)
    def _():
        far(2, 0)

    @pl.when(z == 1)
    def _():
        far(2, 0, 1)

    far(3, 0)

    loads[5].wait()
    for h in range(heads):
        side = slice(h * dim, (h + 1) * dim)
        q, k, v = q_ref[:, side], k_ref[:, side], v_ref[:, side]
        gap = jnp.minimum(cols[h][:, :1] - running[h : h + 1], 0.0)
        table = jnp.where(causal, jnp.exp(gap), 0.0) * scale
        scores = dot(q, k, ((1,), (1,)))
        within[:, side] = jnp.dot(
            (scores * table).astype(bf16), v, preferred_element_type=f32
        )
        grown[h] = jnp.exp(cols[h])

    carry[...] = jnp.zeros_like(carry)
    reach[...] = jnp.zeros_like(reach)
    for k in (1, 2, 3):

        @pl.when(z >= k)
        def _():
            arrived(plane_in.at[z - k], pl_recv.at[z - k])
            carry[...] += jnp.exp(reach[...]) * plane_in[z - k, :dim].astype(f32)
            reach[...] += join_total(plane_in[z - k, dim:])

    entry = carry[...]
    for m in range(4):
        entry_out[m] = entry.astype(bf16)
        if m < 3:
            entry = entry * jnp.exp(totals[m]) + states[m]
    for d in (1, 2, 3):
        copy(
            entry_out.at[beside[d]],
            entry_in.at[n],
            en_send.at[d - 1],
            en_recv.at[d - 1],
            at(z, beside[d], c),
        ).start()
    entry_in[n] = entry_out[n]

    relay(0, 0)
    push(1, 0)

    for d in (1, 2, 3):
        arrived(entry_in.at[beside[d]], en_recv.at[d - 1])
    for load in loads[6:]:
        load.wait()
    for h in range(heads):
        side = slice(h * dim, (h + 1) * dim)
        carried = jnp.dot(q_ref[:, side], entry_in[h], preferred_element_type=f32)
        retained = within[:, side] + carried * grown[h]
        center = jnp.mean(retained, axis=-1, keepdims=True)
        away = retained - center
        spread = jnp.mean(away * away, axis=-1, keepdims=True)
        normed = away * lax.rsqrt(spread + epsilon) * head_gain_ref[side][None].astype(f32)
        gate = gate_ref[:, side].astype(f32)
        mixed[:, side] = (jax.nn.silu(gate) * normed).astype(bf16)

    half = count // 2
    give = pl.ds(pl.multiple_of(other * half, half), half)
    keep = pl.ds(pl.multiple_of(c * half, half), half)
    term_out[...] = jnp.dot(
        mixed[give], out_weight_ref[...], preferred_element_type=f32
    ).astype(bf16)
    copy(term_out, term_in, term_sem.at[0], term_sem.at[1], mate).start()
    kept = jnp.dot(mixed[keep], out_weight_ref[...], preferred_element_type=f32)
    residual[...] = stream_ref[...].astype(f32) + kept.astype(bf16).astype(f32)
    arrived(term_in, term_sem.at[1])
    total = residual[...] + term_in[...].astype(f32)
    residual[...] = total
    mean = jnp.mean(total * total, axis=-1, keepdims=True)
    rows[z, c] = (
        total * lax.rsqrt(mean + epsilon) * norm_gain_ref[...][None].astype(f32)
    ).astype(bf16)

    pieces = PIECES
    high = half // pieces

    def strip(p):
        return pl.ds(p * high, high)

    def pass_on(zz, way, p):
        piece = rows.at[zz, c, strip(p)]
        copy(
            piece,
            piece,
            row_send.at[way, zz, p],
            row_recv.at[min(way, 1), zz, p],
            (mate, at(z + inner, n, c), at(z - inner, n, c))[way],
        ).start()

    def from_outer():
        @pl.when(middle)
        def _():
            zz = z - inner
            for p in range(pieces):
                arrived(rows.at[zz, c, strip(p)], row_recv.at[1, zz, p])
                pass_on(zz, 1, p)
                pass_on(zz, 0, p)

    def from_inner(k, *parts):
        def go():
            zz = z + inner * k
            for p in parts:
                arrived(rows.at[zz, c, strip(p)], row_recv.at[1, zz, p])
                if k < 3:

                    @pl.when(middle)
                    def _():
                        pass_on(zz, 2, p)

                pass_on(zz, 0, p)

        if k < 3:
            go()
        else:
            pl.when(edge)(go)

    for p in range(pieces):
        pass_on(z, 1, p)

        @pl.when(middle)
        def _():
            pass_on(z, 2, p)

        pass_on(z, 0, p)

    relay(1, 0)
    push(2, 0)
    relay(2, 0)
    push(3, 0)
    from_outer()

    @pl.when(edge)
    def _():
        far(1, 1)
        early(0)
        early(1)

    from_inner(1, 0, 1, 2, 3)
    relay(3, 0)
    push(0, 1)

    @pl.when(middle)
    def _():
        push(1, 1)

    from_inner(2, 0, 1)
    for d in range(4):
        finish(d, 0)

    depth = rows.shape[3]

    def raise_rows(j):
        zt = z + inner * jnp.where(edge, j, (0, -1, 1, 2)[j])
        for p in range(pieces):
            arrived(rows.at[zt, other, strip(p)], row_recv.at[0, zt, p])
        both = jnp.dot(
            rows[zt].reshape(count, depth),
            wide[...].reshape(depth, 2 * units),
            preferred_element_type=f32,
        )
        hidden[zt] = (jax.nn.silu(both[:, :units]) * both[:, units:]).astype(bf16)

    raise_rows(0)
    from_inner(2, 2)
    raise_rows(1)
    relay(0, 1)

    from_inner(2, 3)

    @pl.when(middle)
    def _():
        for p in range(pieces):
            left(rows.at[0, 0, strip(0)], row_send.at[1, z - inner, p])
        far(2, 1)
        onward(0)

    raise_rows(2)
    from_inner(3, 0, 1, 2, 3)
    raise_rows(3)

    @pl.when(middle)
    def _():
        far(1, 1)
        relay(1, 1)

    def turn(j):
        return z + inner * jnp.where(
            edge, 3 - j, jnp.where(j == 2, -1, jnp.where(j == 3, 0, j + 1))
        )

    def send_sum(zt, p, to, side):
        copy(
            sum_out.at[zt, p],
            sum_in.at[side, zt, p],
            sum_send.at[zt, p],
            sum_recv.at[side, zt, p],
            to,
        ).start()

    def lower(q):
        p = level[1][q]
        weight = jnp.concatenate([down[p * 4 + m] for m in range(4)], axis=1)

        def product(j, carried):
            zt = turn(j)
            out = jnp.dot(hidden[zt], weight, preferred_element_type=f32).astype(bf16)
            part_own[zt, p, 0] = out[:half]
            part_own[zt, p, 1] = out[half:]
            copy(
                part_own.at[zt, p, other],
                part_in.at[zt, p],
                part_sem.at[zt, p],
                part_recv.at[zt, p],
                mate,
            ).start()
            return carried

        def gather(j, carried):
            zt = turn(j)
            arrived(part_in.at[zt, p], part_recv.at[zt, p])
            both = part_own[zt, p, c].astype(f32) + part_in[zt, p].astype(f32)
            sum_own[zt, p] = both

            @pl.when(edge & (zt != z))
            def _():
                sum_out[zt, p] = both.astype(bf16)

            @pl.when(edge & (j < (3 if q < 2 else 2)))
            def _():
                send_sum(zt, p, at(z + inner, n, c), 0)

            return carried

        lax.fori_loop(0, GROUP, product, 0)
        lax.fori_loop(0, GROUP, gather, 0)

    def add_on(zt, p, side, to):
        arrived(sum_in.at[side, zt, p], sum_recv.at[side, zt, p])
        sum_out[zt, p] = (sum_own[zt, p] + sum_in[side, zt, p].astype(f32)).astype(bf16)
        send_sum(zt, p, to, 1)

    def inward(i):
        p = flip(z - inner, i)
        add_on(z + 2 * inner, p, 0, at(z + inner, n, c))
        add_on(z + inner, p, 0, at(z + inner, n, c))

    def outward(i):
        p = flip(z + 2 * inner, i)
        add_on(z - inner, p, 1, at(z - inner, n, c))

    @pl.when(edge)
    def _():
        push(1, 1)

    finish(0, 1)
    lower(0)

    @pl.when(edge)
    def _():
        relay(1, 1)

    push(2, 1)
    finish(1, 1)
    lower(1)

    @pl.when(middle)
    def _():
        left(given[1].at[0], w_far.at[1, 0])
        far(3, 1)
        onward(1)

    push(3, 1)
    relay(2, 1)
    relay(3, 1)

    @pl.when(middle)
    def _():
        inward(0)

    finish(2, 1)
    lower(2)
    finish(3, 1)
    lower(3)

    @pl.when(edge)
    def _():
        for q in (2, 3):
            send_sum(z + inner, level[1][q], at(z + inner, n, c), 0)

    @pl.when(middle)
    def _():
        inward(1)
        outward(0)
        outward(1)
        inward(2)
        outward(2)
        inward(3)
        outward(3)

    wide_step = depth // GROUP
    for p in range(GROUP):
        side = slice(p * wide_step, (p + 1) * wide_step)
        residual[:, side] += sum_own[z, p]

        @pl.when(middle)
        def _():
            arrived(sum_in.at[0, z, p], sum_recv.at[0, z, p])
            residual[:, side] += sum_in[0, z, p].astype(f32)

    stores = []
    for p in range(GROUP):
        side = slice(p * wide_step, (p + 1) * wide_step)
        arrived(sum_in.at[1, z, p], sum_recv.at[1, z, p])
        result[:, side] = (
            residual[:, side] + sum_in[1, z, p].astype(f32)
        ).astype(result.dtype)
        stores.append(
            pltpu.make_async_copy(result.at[:, side], result_ref.at[:, side], out_sem.at[p])
        )
        stores[p].start()

    settle_weights()
    for store in stores:
        store.wait()
    for d in (1, 2, 3):
        left(state_out.at[0], st_send.at[d - 1])
        left(entry_out.at[0], en_send.at[d - 1])
        for p in range(GROUP):
            left(sum_out.at[0, 0], sum_send.at[flip(z, d), p])

        @pl.when(z + d <= 3)
        def _():
            left(plane_out, pl_send.at[d - 1])

    left(term_out, term_sem.at[0])

    @pl.when(middle)
    def _():
        for k in range(2):
            left(transit.at[0], transit_send.at[k])

    for zz in range(GROUP):
        for p in range(GROUP):
            left(part_in.at[0, 0], part_sem.at[zz, p])
        for p in range(pieces):
            left(rows.at[0, 0, strip(0)], row_send.at[0, zz, p])
    for p in range(pieces):
        left(rows.at[0, 0, strip(0)], row_send.at[1, z, p])

        @pl.when(middle)
        def _():
            for k in range(3):
                left(rows.at[0, 0, strip(0)], row_send.at[2, z + inner * k, p])


def split_total(total, line):
    top = total.astype(bf16).astype(f32)
    mid = (total - top).astype(bf16).astype(f32)
    low = total - top - mid
    return jnp.where(line == 0, top, jnp.where(line == 1, mid, low)).astype(bf16)


def join_total(parts):
    parts = parts.astype(f32)
    return parts[0:1] + parts[1:2] + parts[2:3]


def fused_local(
    stream,
    queries,
    keys_in,
    values_in,
    gate_in,
    log_decay,
    head_gain,
    out_weight,
    norm_gain,
    gate_weight,
    up_weight,
    down_weight,
):
    count, heads = log_decay.shape
    width = queries.shape[1]
    dim = width // heads
    depth = stream.shape[1]
    own, units = gate_weight.shape
    sizes = GROUP * GROUP
    part = units // GROUP
    down = down_weight.reshape(GROUP, part, down_weight.shape[1])
    half = count // 2
    vmem = pltpu.VMEM
    dma = pltpu.SemaphoreType.DMA
    given = (
        stream,
        queries,
        keys_in,
        values_in,
        gate_in,
        log_decay.T,
        head_gain,
        out_weight,
        norm_gain,
        gate_weight,
        up_weight,
    )
    return pl.pallas_call(
        layer_kernel,
        out_shape=jax.ShapeDtypeStruct((half, depth), bf16),
        in_specs=[pl.BlockSpec(memory_space=pl.ANY)] * 12,
        out_specs=pl.BlockSpec(memory_space=pl.ANY),
        scratch_shapes=[
            *(vmem(value.shape, value.dtype) for value in given),
            vmem((GROUP, own, 2 * part), bf16),
            vmem((sizes, own, 2 * part), bf16),
            vmem((sizes, part, down_weight.shape[1]), bf16),
            vmem((2, part, down_weight.shape[1]), bf16),
            vmem((GROUP, 2, half, depth), bf16),
            vmem((half, depth), f32),
            vmem((heads, count, dim), f32),
            vmem((count, width), f32),
            vmem((heads, dim + TAIL, dim), bf16),
            vmem((heads, dim + TAIL, dim), bf16),
            vmem((dim + TAIL, dim), bf16),
            vmem((GROUP, dim + TAIL, dim), bf16),
            vmem((dim, dim), f32),
            vmem((1, dim), f32),
            vmem((heads, dim, dim), bf16),
            vmem((heads, dim, dim), bf16),
            vmem((count, width), bf16),
            vmem((half, depth), bf16),
            vmem((half, depth), bf16),
            vmem((GROUP, count, part), bf16),
            vmem((GROUP, GROUP, 2, half, depth // GROUP), bf16),
            vmem((GROUP, GROUP, half, depth // GROUP), bf16),
            vmem((GROUP, GROUP, half, depth // GROUP), f32),
            vmem((GROUP, GROUP, half, depth // GROUP), bf16),
            vmem((2, GROUP, GROUP, half, depth // GROUP), bf16),
            vmem((half, depth), bf16),
            dma((12,)),
            dma((GROUP,)),
            dma((2, GROUP, 2)),
            dma((2, GROUP, 2)),
            dma((2, sizes, 2)),
            dma((2, GROUP - 1)),
            dma((2,)),
            dma((2,)),
            dma((3,)),
            dma((3,)),
            dma((3,)),
            dma((GROUP,)),
            dma((3,)),
            dma((3,)),
            dma((2,)),
            dma((3, GROUP, PIECES)),
            dma((2, GROUP, PIECES)),
            dma((GROUP, GROUP)),
            dma((GROUP, GROUP)),
            dma((GROUP, GROUP)),
            dma((2, GROUP, GROUP)),
        ],
        compiler_params=pltpu.CompilerParams(
            collective_id=0, has_side_effects=True, vmem_limit_bytes=60 * 1024 * 1024
        ),
        name="layer",
    )(*given, down)


def fused(mesh):
    return jax.shard_map(
        fused_local,
        mesh=mesh,
        in_specs=(
            P(("sp", "tp"), None),
            P("sp", "tp"),
            P("sp", "tp"),
            P("sp", "tp"),
            P("sp", "tp"),
            P("sp", "tp"),
            P("tp"),
            P("tp", None),
            P(),
            P("sp", "tp"),
            P("sp", "tp"),
            P("tp", "sp"),
        ),
        out_specs=P(("sp", "tp"), None),
        check_vma=False,
    )


def solution(mesh):
    if fits(mesh):
        return fused(mesh)
    devices = mesh.devices
    count, pair = devices.shape
    split = Mesh(devices.reshape(GROUP, count // GROUP, pair), (*SP, "tp"))
    return jax.shard_map(
        local,
        mesh=split,
        in_specs=(
            P((*SP, "tp"), None),
            P(SP, "tp"),
            P(SP, "tp"),
            P(SP, "tp"),
            P(SP, "tp"),
            P(SP, "tp"),
            P("tp"),
            P("tp", None),
            P(),
            P(SP, "tp"),
            P(SP, "tp"),
            P("tp", SP),
        ),
        out_specs=P((*SP, "tp"), None),
        check_vma=False,
    )
```

```python
import functools

import jax
import jax.numpy as jnp
from jax import lax
from jax.experimental import pallas as pl
from jax.experimental.pallas import tpu as pltpu
from jax.sharding import Mesh, PartitionSpec as P

epsilon = 1e-06
GROUP = 4
SP = ("far", "near")
f32, bf16 = jnp.float32, jnp.bfloat16


def swap(value, axis, bits):
    size = lax.axis_size(axis)
    return lax.ppermute(value, axis, [(i, i ^ bits) for i in range(size)])


def near_blocks(value):
    size = lax.axis_size("near")
    steps = (1, 2) if size == 4 else range(1, size)
    return [value] + [swap(value, "near", s) for s in steps]


def near_rest(blocks):
    half = blocks[0].shape[0] // 2
    cut = [(block[:half], block[half:]) for block in blocks]
    if lax.axis_size("near") == 4:
        cut.append((swap(cut[1][0], "near", 2), swap(cut[2][1], "near", 1)))
    return cut


def spread_weights(gate_weight, up_weight, down_weight):
    groups = lax.axis_size("far")
    far_at = lax.axis_index("far")
    width = gate_weight.shape[1] // groups
    all_rows, all_columns = [], []
    for s in range(groups):
        at = (far_at ^ s) * width
        rows = jnp.concatenate(
            [
                lax.dynamic_slice_in_dim(gate_weight, at, width, 1),
                lax.dynamic_slice_in_dim(up_weight, at, width, 1),
            ],
            axis=0,
        )
        all_rows.append(swap(rows, "far", s) if s else rows)
    for s in range(groups):
        at = (far_at ^ s) * width
        all_columns.append(lax.dynamic_slice_in_dim(down_weight, at, width, 0))
    return [near_blocks(piece) for piece in all_rows], all_columns


def by_distance(value):
    groups, near = lax.axis_size("far"), lax.axis_size("near")
    here = lax.axis_index("far") * near + lax.axis_index("near")
    width = value.shape[1] // (groups * near)
    return jnp.concatenate(
        [
            lax.dynamic_slice_in_dim(value, (here ^ k) * width, width, 1)
            for k in range(groups * near)
        ],
        axis=1,
    )


def turned(value, bits):
    groups = lax.axis_size("far")
    width = value.shape[1] // groups
    return jnp.concatenate(
        [value[:, (g ^ bits) * width : ((g ^ bits) + 1) * width] for g in range(groups)], axis=1
    )


def gather_pair(rows):
    if lax.axis_size("tp") == 2:
        return jnp.concatenate([rows, swap(rows, "tp", 1)], axis=0)
    return lax.all_gather(rows, "tp", axis=0, tiled=True)


def scatter_pair(terms):
    terms = terms.astype(bf16)
    if lax.axis_size("tp") == 2:
        half = terms.shape[0] // 2
        return terms[:half].astype(f32) + swap(terms[half:], "tp", 1).astype(f32)
    return lax.psum_scatter(terms, "tp", scatter_dimension=0, tiled=True).astype(f32)


def dot(a, b, dims=((1,), (0,))):
    return lax.dot_general(a, b, (dims, ((), ())), preferred_element_type=f32)


def retention(queries, keys_in, values_in, log_decay):
    row_count, heads = log_decay.shape
    dim = queries.shape[1] // heads
    scale = dim ** (-0.5)
    running = jnp.cumsum(log_decay, axis=0)
    total = running[-1]
    offsets = jnp.arange(row_count)
    causal = offsets[:, None] >= offsets[None, :]
    within, states = [], []
    for h in range(heads):
        cut = slice(h * dim, (h + 1) * dim)
        q, k, v = queries[:, cut], keys_in[:, cut], values_in[:, cut]
        col = running[:, h]
        gap = jnp.minimum(col[:, None] - col[None, :], 0.0)
        table = jnp.where(causal, jnp.exp(gap), 0.0) * scale
        within.append(dot((dot(q, k, ((1,), (1,))) * table).astype(bf16), v))
        tail = (jnp.exp(total[h] - col) * scale)[:, None]
        states.append(dot((k.astype(f32) * tail).astype(bf16), v, ((0,), (0,))))
    return running, total, within, jnp.concatenate(states, axis=0)


def incoming_states(total, state, columns):
    heads = total.shape[0]
    near = lax.axis_size("near")
    here = lax.axis_index("far") * near + lax.axis_index("near")
    high = lax.reduce_precision(total, 8, 7)
    mid = lax.reduce_precision(total - high, 8, 7)
    low = total - high - mid
    parts = jnp.concatenate([high, mid, low])
    extra = -(-parts.shape[0] // 16) * 16
    parts = jnp.pad(parts, (0, extra - parts.shape[0]))
    width = state.shape[1]
    packed = jnp.concatenate(
        [state.astype(bf16), jnp.broadcast_to(parts[:, None], (extra, width)).astype(bf16)], axis=0
    )
    everything = lax.all_gather(packed, SP)
    everything, columns = lax.optimization_barrier((everything, columns))
    columns = [swap(piece, "far", s) if s else piece for s, piece in enumerate(columns)]
    count = everything.shape[0]
    logs = everything[:, state.shape[0] : state.shape[0] + 3 * heads, 0].astype(f32)
    logs = logs.reshape(count, 3, heads).sum(axis=1)
    index = jnp.arange(count)
    between = (index[None, :] > index[:, None]) & (index[None, :] < here)
    reach = jnp.sum(jnp.where(between[:, :, None], logs[None], 0.0), axis=1)
    factor = jnp.where((index < here)[:, None], jnp.exp(reach), 0.0)
    states = everything[:, : state.shape[0]].reshape(count, heads, -1, width)
    return jnp.sum(factor[:, :, None, None] * states.astype(f32), axis=0), columns


def local(
    stream,
    queries,
    keys_in,
    values_in,
    gate_in,
    log_decay,
    head_gain,
    out_weight,
    norm_gain,
    gate_weight,
    up_weight,
    down_weight,
):
    weight_rows, weight_columns = spread_weights(gate_weight, up_weight, down_weight)
    heads = log_decay.shape[1]
    dim = queries.shape[1] // heads
    running, total, within, state = retention(queries, keys_in, values_in, log_decay)
    incoming, weight_columns = incoming_states(total, state, weight_columns)
    mixed = []
    for h in range(heads):
        cut = slice(h * dim, (h + 1) * dim)
        carried = dot(queries[:, cut], incoming[h].astype(bf16))
        retained = within[h] + carried * jnp.exp(running[:, h])[:, None]
        center = jnp.mean(retained, axis=-1, keepdims=True)
        spread = jnp.mean(jnp.square(retained - center), axis=-1, keepdims=True)
        normed = (retained - center) * lax.rsqrt(spread + epsilon) * head_gain[cut].astype(f32)
        mixed.append((jax.nn.silu(gate_in[:, cut].astype(f32)) * normed).astype(bf16))
    terms = dot(jnp.concatenate(mixed, axis=1), out_weight).astype(bf16)
    if lax.axis_size("tp") == 2:
        half = terms.shape[0] // 2
        mine = lax.axis_index("tp") * half
        sent = swap(lax.dynamic_slice_in_dim(terms, half - mine, half, 0), "tp", 1)
        kept = lax.dynamic_slice_in_dim(terms, mine, half, 0)
        attended = kept.astype(f32) + sent.astype(f32)
    else:
        attended = scatter_pair(terms)
    residual = stream.astype(f32) + attended
    normed = (
        residual
        * lax.rsqrt(jnp.mean(residual * residual, axis=-1, keepdims=True) + epsilon)
        * norm_gain.astype(f32)
    ).astype(bf16)

    normed = by_distance(normed)
    normed, weight_rows, weight_columns = lax.optimization_barrier(
        (normed, weight_rows, weight_columns)
    )
    weight_rows = [block for piece in weight_rows for block in near_rest(piece)]
    weight_columns = [
        block for piece in weight_columns for block in near_rest(near_blocks(piece))
    ]
    groups = lax.axis_size("far")
    arrived = [normed] + [swap(normed, "far", s) for s in range(1, groups)]
    rows = [turned(gather_pair(piece), s) for s, piece in enumerate(arrived)]
    gate_full = jnp.concatenate([gate for gate, _ in weight_rows], axis=0)
    up_full = jnp.concatenate([up for _, up in weight_rows], axis=0)
    down_full = jnp.concatenate(
        [jnp.concatenate([part[i] for part in weight_columns], axis=1) for i in range(2)], axis=0
    )
    together = jnp.concatenate(rows, axis=0)
    hidden = (jax.nn.silu(dot(together, gate_full)) * dot(together, up_full)).astype(bf16)
    height = rows[0].shape[0]
    mixer_out = 0.0
    for s in (*range(1, groups), 0):
        part = scatter_pair(dot(hidden[s * height : (s + 1) * height], down_full))
        if s:
            part = turned(swap(part.astype(bf16), "far", s).astype(f32), s)
        mixer_out = mixer_out + part
    return (residual + by_distance(mixer_out)).astype(bf16)


MESH = pl.DeviceIdType.MESH
HIGHEST = lax.Precision.HIGHEST
TAIL = 16
PIECES = 4


def fits(mesh):
    return mesh.shape["tp"] == 2 and mesh.shape["sp"] == GROUP * GROUP


def flip(v, d):
    if d == 0:
        return v
    if d == 1:
        return v + 1 - 2 * lax.rem(v, 2)
    if d == 2:
        return lax.rem(v + 2, 4)
    return 3 - v


def layer_kernel(
    stream_in,
    q_in,
    k_in,
    v_in,
    gate_in,
    decay_in,
    head_gain_in,
    out_weight_in,
    norm_gain_in,
    gate_weight_in,
    up_weight_in,
    down_in,
    result_ref,
    stream_ref,
    q_ref,
    k_ref,
    v_ref,
    gate_ref,
    decay_ref,
    head_gain_ref,
    out_weight_ref,
    norm_gain_ref,
    gate_weight_ref,
    up_weight_ref,
    wide_own,
    wide,
    down,
    transit,
    rows,
    residual,
    grown,
    within,
    state_out,
    state_in,
    plane_out,
    plane_in,
    carry,
    reach,
    entry_out,
    entry_in,
    mixed,
    term_out,
    term_in,
    hidden,
    part_own,
    part_in,
    sum_own,
    sum_out,
    sum_in,
    result,
    in_sem,
    out_sem,
    w_send,
    w_relay,
    w_recv,
    w_far,
    transit_send,
    transit_recv,
    st_send,
    st_recv,
    pl_send,
    pl_recv,
    en_send,
    en_recv,
    term_sem,
    row_send,
    row_recv,
    part_sem,
    part_recv,
    sum_send,
    sum_recv,
):
    sp, c = lax.axis_index("sp"), lax.axis_index("tp")
    z, n = lax.div(sp, 4), lax.rem(sp, 4)
    other = 1 - c
    beside = [flip(n, d) for d in range(4)]
    inner = jnp.where(z < 2, 1, -1)
    middle = (z == 1) | (z == 2)
    edge = (z == 0) | (z == 3)
    ends = [jnp.where(edge, flip(z, d), flip(z, 5 - d)) for d in (2, 3)]
    level = (
        [flip(z, d) for d in (0, 1, 3, 2)],
        [z, flip(z, 1), *ends],
    )

    def at(zz, nn, cc):
        return (zz * 4 + nn, cc)

    mate = at(z, n, other)

    def copy(src, dst, send, recv, to):
        return pltpu.make_async_remote_copy(
            src_ref=src,
            dst_ref=dst,
            send_sem=send,
            recv_sem=recv,
            device_id=to,
            device_id_type=MESH,
        )

    def arrived(ref, recv):
        copy(ref, ref, recv, recv, mate).wait_recv()

    def left(ref, send):
        copy(ref, ref, send, send, mate).wait_send()

    loads = [
        pltpu.make_async_copy(src, dst, in_sem.at[i])
        for i, (src, dst) in enumerate(
            (
                (decay_in, decay_ref),
                (k_in, k_ref),
                (v_in, v_ref),
                (gate_weight_in, gate_weight_ref),
                (up_weight_in, up_weight_ref),
                (q_in, q_ref),
                (down_in.at[z], down.at[sp]),
                (gate_in, gate_ref),
                (head_gain_in, head_gain_ref),
                (out_weight_in, out_weight_ref),
                (stream_in, stream_ref),
                (norm_gain_in, norm_gain_ref),
            )
        )
    ]
    for load in loads:
        load.start()

    barrier = pltpu.get_barrier_semaphore()
    partners = [mate]
    partners += [at(z, beside[d], c) for d in (1, 2, 3)]
    partners += [at(flip(z, d), n, c) for d in (1, 2, 3)]
    for to in partners:
        pl.semaphore_signal(barrier, inc=1, device_id=to, device_id_type=MESH)

    units = down.shape[1]
    heads = decay_ref.shape[0]
    dim = q_ref.shape[1] // heads
    count = q_ref.shape[0]
    scale = dim ** (-0.5)
    loads[0].wait()
    decay = decay_ref[...]
    low = lax.broadcasted_iota(jnp.int32, (count, count), 0)
    high = lax.broadcasted_iota(jnp.int32, (count, count), 1)
    causal = low >= high
    running = jnp.dot(
        decay, (low <= high).astype(f32), precision=HIGHEST, preferred_element_type=f32
    )
    line = lax.broadcasted_iota(jnp.int32, (TAIL, dim), 0)
    loads[1].wait()
    loads[2].wait()
    cols = []
    for h in range(heads):
        side = slice(h * dim, (h + 1) * dim)
        col = jnp.broadcast_to(running[h : h + 1], (dim, count)).T
        cols.append(col)
        total = running[h : h + 1, count - 1 : count]
        tail = jnp.exp(total - col) * scale
        keyed = (k_ref[:, side].astype(f32) * tail).T.astype(bf16)
        state = jnp.dot(keyed, v_ref[:, side], preferred_element_type=f32)
        state_out[h, :dim] = state.astype(bf16)
        state_out[h, dim:] = split_total(total, line)

    loads[3].wait()
    loads[4].wait()
    for g in range(wide_own.shape[0]):
        side = slice(g * units, (g + 1) * units)
        wide_own[g] = jnp.concatenate(
            [gate_weight_ref[:, side], up_weight_ref[:, side]], axis=1
        )
    pl.semaphore_wait(barrier, len(partners))

    full = (wide, down)
    given = (wide_own, down_in)
    cut = (wide.shape[1] // 2, down.shape[1] // 2)

    def far(d, kind, part=None):
        half = cut[kind]
        some = pl.ds(0, 2 * half) if part is None else pl.ds(part * half, half)
        copy(
            given[kind].at[level[kind][d], some],
            full[kind].at[sp, some],
            w_far.at[kind, d - 1],
            w_recv.at[kind, sp, 0],
            at(level[kind][d], n, c),
        ).start()

    def early(k):
        copy(
            down_in.at[z + inner * (k + 2)],
            transit.at[k],
            w_far.at[1, k + 1],
            transit_recv.at[k],
            at(z + inner, n, c),
        ).start()

    def onward(k):
        arrived(transit.at[k], transit_recv.at[k])
        slot = (z - inner) * 4 + n
        copy(
            transit.at[k],
            down.at[slot],
            transit_send.at[k],
            w_recv.at[1, slot, 0],
            at(z + inner * (k + 1), n, c),
        ).start()

    def push(d, kind):
        slot = level[kind][d] * 4 + n
        if d:
            arrived(full[kind].at[slot], w_recv.at[kind, slot, 0])
        src = full[kind].at[slot] if d else given[kind].at[z]
        for a in (1, 2):
            copy(
                src,
                full[kind].at[slot],
                w_send.at[kind, a - 1],
                w_recv.at[kind, slot, 0],
                at(z, beside[a], c),
            ).start()

    def relay(d, kind):
        half = cut[kind]
        for a in (1, 2):
            slot = level[kind][d] * 4 + beside[a]
            arrived(full[kind].at[slot], w_recv.at[kind, slot, 0])
            part = pl.ds(0, half) if a == 1 else pl.ds(half, half)
            piece = full[kind].at[slot, part]
            copy(
                piece,
                piece,
                w_relay.at[kind, a - 1],
                w_recv.at[kind, slot, a - 1],
                at(z, beside[3 - a], c),
            ).start()

    def finish(d, kind):
        half = cut[kind]
        slot = level[kind][d] * 4 + beside[3]
        arrived(full[kind].at[slot, pl.ds(0, half)], w_recv.at[kind, slot, 0])
        arrived(full[kind].at[slot, pl.ds(half, half)], w_recv.at[kind, slot, 1])

    def settle_weights():
        for kind in (0, 1):
            for d in range(4):
                if (kind, d) == (1, 1):

                    @pl.when(edge)
                    def _():
                        left(given[kind].at[0], w_far.at[kind, d - 1])

                elif d:
                    left(given[kind].at[0], w_far.at[kind, d - 1])
            for a in (0, 1):
                left(given[kind], w_send.at[kind, a])
                left(given[kind].at[pl.ds(0, 2)], w_relay.at[kind, a])

    for d in (1, 2, 3):
        copy(
            state_out.at[beside[d]],
            state_in.at[n],
            st_send.at[d - 1],
            st_recv.at[d - 1],
            at(z, beside[d], c),
        ).start()
    state_in[n] = state_out[n]
    push(0, 0)
    far(1, 0, 0)

    @pl.when(z == 1)
    def _():
        far(2, 0, 0)

    @pl.when(z == 2)
    def _():
        far(2, 0)

    wide[sp] = wide_own[z]

    for d in (1, 2, 3):
        arrived(state_in.at[beside[d]], st_recv.at[d - 1])
    totals = [join_total(state_in[m, dim:]) for m in range(4)]
    states = [state_in[m, :dim].astype(f32) for m in range(4)]
    plane, span = states[0], totals[0]
    for m in range(1, 4):
        plane = plane * jnp.exp(totals[m]) + states[m]
        span = span + totals[m]
    plane_out[:dim] = plane.astype(bf16)
    plane_out[dim:] = split_total(span, line)
    for k in (1, 2, 3):

        @pl.when(z + k <= 3)
        def _():
            copy(
                plane_out,
                plane_in.at[z],
                pl_send.at[k - 1],
                pl_recv.at[z],
                at(z + k, n, c),
            ).start()

    far(1, 0, 1)

    @pl.when(edge)
    def _():
        far(2, 0)

    @pl.when(z == 1)
    def _():
        far(2, 0, 1)

    far(3, 0)

    loads[5].wait()
    for h in range(heads):
        side = slice(h * dim, (h + 1) * dim)
        q, k, v = q_ref[:, side], k_ref[:, side], v_ref[:, side]
        gap = jnp.minimum(cols[h][:, :1] - running[h : h + 1], 0.0)
        table = jnp.where(causal, jnp.exp(gap), 0.0) * scale
        scores = dot(q, k, ((1,), (1,)))
        within[:, side] = jnp.dot(
            (scores * table).astype(bf16), v, preferred_element_type=f32
        )
        grown[h] = jnp.exp(cols[h])

    carry[...] = jnp.zeros_like(carry)
    reach[...] = jnp.zeros_like(reach)
    for k in (1, 2, 3):

        @pl.when(z >= k)
        def _():
            arrived(plane_in.at[z - k], pl_recv.at[z - k])
            carry[...] += jnp.exp(reach[...]) * plane_in[z - k, :dim].astype(f32)
            reach[...] += join_total(plane_in[z - k, dim:])

    entry = carry[...]
    for m in range(4):
        entry_out[m] = entry.astype(bf16)
        if m < 3:
            entry = entry * jnp.exp(totals[m]) + states[m]
    for d in (1, 2, 3):
        copy(
            entry_out.at[beside[d]],
            entry_in.at[n],
            en_send.at[d - 1],
            en_recv.at[d - 1],
            at(z, beside[d], c),
        ).start()
    entry_in[n] = entry_out[n]

    relay(0, 0)
    push(1, 0)

    for d in (1, 2, 3):
        arrived(entry_in.at[beside[d]], en_recv.at[d - 1])
    for load in loads[6:]:
        load.wait()
    for h in range(heads):
        side = slice(h * dim, (h + 1) * dim)
        carried = jnp.dot(q_ref[:, side], entry_in[h], preferred_element_type=f32)
        retained = within[:, side] + carried * grown[h]
        center = jnp.mean(retained, axis=-1, keepdims=True)
        away = retained - center
        spread = jnp.mean(away * away, axis=-1, keepdims=True)
        normed = away * lax.rsqrt(spread + epsilon) * head_gain_ref[side][None].astype(f32)
        gate = gate_ref[:, side].astype(f32)
        mixed[:, side] = (jax.nn.silu(gate) * normed).astype(bf16)

    half = count // 2
    give = pl.ds(pl.multiple_of(other * half, half), half)
    keep = pl.ds(pl.multiple_of(c * half, half), half)
    term_out[...] = jnp.dot(
        mixed[give], out_weight_ref[...], preferred_element_type=f32
    ).astype(bf16)
    copy(term_out, term_in, term_sem.at[0], term_sem.at[1], mate).start()
    kept = jnp.dot(mixed[keep], out_weight_ref[...], preferred_element_type=f32)
    residual[...] = stream_ref[...].astype(f32) + kept.astype(bf16).astype(f32)
    arrived(term_in, term_sem.at[1])
    total = residual[...] + term_in[...].astype(f32)
    residual[...] = total
    mean = jnp.mean(total * total, axis=-1, keepdims=True)
    rows[z, c] = (
        total * lax.rsqrt(mean + epsilon) * norm_gain_ref[...][None].astype(f32)
    ).astype(bf16)

    pieces = PIECES
    high = half // pieces

    def strip(p):
        return pl.ds(p * high, high)

    def pass_on(zz, way, p):
        piece = rows.at[zz, c, strip(p)]
        copy(
            piece,
            piece,
            row_send.at[way, zz],
            row_recv.at[min(way, 1), zz, p],
            (mate, at(z + inner, n, c), at(z - inner, n, c))[way],
        ).start()

    def from_outer():
        @pl.when(middle)
        def _():
            zz = z - inner
            for p in range(pieces):
                arrived(rows.at[zz, c, strip(p)], row_recv.at[1, zz, p])
                pass_on(zz, 1, p)
                pass_on(zz, 0, p)

    def from_inner(k, *parts):
        def go():
            zz = z + inner * k
            for p in parts:
                arrived(rows.at[zz, c, strip(p)], row_recv.at[1, zz, p])
                if k < 3:

                    @pl.when(middle)
                    def _():
                        pass_on(zz, 2, p)

                pass_on(zz, 0, p)

        if k < 3:
            go()
        else:
            pl.when(edge)(go)

    for p in range(pieces):
        pass_on(z, 1, p)

        @pl.when(middle)
        def _():
            pass_on(z, 2, p)

        pass_on(z, 0, p)

    relay(1, 0)
    push(2, 0)
    relay(2, 0)
    push(3, 0)
    from_outer()

    @pl.when(edge)
    def _():
        far(1, 1)
        early(0)
        early(1)

    from_inner(1, 0, 1, 2, 3)
    relay(3, 0)
    push(0, 1)

    @pl.when(middle)
    def _():
        push(1, 1)

    from_inner(2, 0, 1)
    for d in range(4):
        finish(d, 0)

    depth = rows.shape[3]

    def raise_rows(j):
        zt = z + inner * jnp.where(edge, j, (0, -1, 1, 2)[j])
        for p in range(pieces):
            arrived(rows.at[zt, other, strip(p)], row_recv.at[0, zt, p])
        both = jnp.dot(
            rows[zt].reshape(count, depth),
            wide[...].reshape(depth, 2 * units),
            preferred_element_type=f32,
        )
        hidden[zt] = (jax.nn.silu(both[:, :units]) * both[:, units:]).astype(bf16)

    raise_rows(0)
    from_inner(2, 2)
    raise_rows(1)
    relay(0, 1)

    from_inner(2, 3)

    @pl.when(middle)
    def _():
        left(rows.at[0, 0], row_send.at[1, z - inner])
        far(2, 1)
        onward(0)

    raise_rows(2)
    from_inner(3, 0, 1, 2, 3)
    raise_rows(3)

    @pl.when(middle)
    def _():
        far(1, 1)
        relay(1, 1)

    def turn(j):
        return z + inner * jnp.where(
            edge, 3 - j, jnp.where(j == 2, -1, jnp.where(j == 3, 0, j + 1))
        )

    def send_sum(zt, p, to, side):
        copy(
            sum_out.at[zt, p],
            sum_in.at[side, zt, p],
            sum_send.at[zt],
            sum_recv.at[side, zt, p],
            to,
        ).start()

    def lower(q):
        p = level[1][q]
        weight = jnp.concatenate([down[p * 4 + m] for m in range(4)], axis=1)

        def product(j, carried):
            zt = turn(j)
            out = jnp.dot(hidden[zt], weight, preferred_element_type=f32).astype(bf16)
            part_own[zt, p, 0] = out[:half]
            part_own[zt, p, 1] = out[half:]
            copy(
                part_own.at[zt, p, other],
                part_in.at[zt, p],
                part_sem.at[zt],
                part_recv.at[zt, p],
                mate,
            ).start()
            return carried

        def gather(j, carried):
            zt = turn(j)
            arrived(part_in.at[zt, p], part_recv.at[zt, p])
            both = part_own[zt, p, c].astype(f32) + part_in[zt, p].astype(f32)
            sum_own[zt, p] = both

            @pl.when(edge & (zt != z))
            def _():
                sum_out[zt, p] = both.astype(bf16)

            @pl.when(edge & (j < (3 if q < 2 else 2)))
            def _():
                send_sum(zt, p, at(z + inner, n, c), 0)

            return carried

        lax.fori_loop(0, GROUP, product, 0)
        lax.fori_loop(0, GROUP, gather, 0)

    def add_on(zt, p, side, to):
        arrived(sum_in.at[side, zt, p], sum_recv.at[side, zt, p])
        sum_out[zt, p] = (sum_own[zt, p] + sum_in[side, zt, p].astype(f32)).astype(bf16)
        send_sum(zt, p, to, 1)

    def inward(i):
        p = flip(z - inner, i)
        add_on(z + 2 * inner, p, 0, at(z + inner, n, c))
        add_on(z + inner, p, 0, at(z + inner, n, c))

    def outward(i):
        p = flip(z + 2 * inner, i)
        add_on(z - inner, p, 1, at(z - inner, n, c))

    @pl.when(edge)
    def _():
        push(1, 1)

    finish(0, 1)
    lower(0)

    @pl.when(edge)
    def _():
        relay(1, 1)

    push(2, 1)
    finish(1, 1)
    lower(1)

    @pl.when(middle)
    def _():
        left(given[1].at[0], w_far.at[1, 0])
        far(3, 1)
        onward(1)

    push(3, 1)
    relay(2, 1)
    relay(3, 1)

    @pl.when(middle)
    def _():
        inward(0)

    finish(2, 1)
    lower(2)
    finish(3, 1)
    lower(3)

    @pl.when(edge)
    def _():
        for q in (2, 3):
            send_sum(z + inner, level[1][q], at(z + inner, n, c), 0)

    @pl.when(middle)
    def _():
        inward(1)
        outward(0)
        outward(1)
        inward(2)
        outward(2)
        inward(3)
        outward(3)

    wide_step = depth // GROUP
    for p in range(GROUP):
        side = slice(p * wide_step, (p + 1) * wide_step)
        residual[:, side] += sum_own[z, p]

        @pl.when(middle)
        def _():
            arrived(sum_in.at[0, z, p], sum_recv.at[0, z, p])
            residual[:, side] += sum_in[0, z, p].astype(f32)

    stores = []
    for p in range(GROUP):
        side = slice(p * wide_step, (p + 1) * wide_step)
        arrived(sum_in.at[1, z, p], sum_recv.at[1, z, p])
        result[:, side] = (
            residual[:, side] + sum_in[1, z, p].astype(f32)
        ).astype(result.dtype)
        stores.append(
            pltpu.make_async_copy(result.at[:, side], result_ref.at[:, side], out_sem.at[p])
        )
        stores[p].start()

    settle_weights()
    for store in stores:
        store.wait()
    for d in (1, 2, 3):
        left(state_out.at[0], st_send.at[d - 1])
        left(entry_out.at[0], en_send.at[d - 1])
        left(sum_out.at[0], sum_send.at[flip(z, d)])

        @pl.when(z + d <= 3)
        def _():
            left(plane_out, pl_send.at[d - 1])

    left(term_out, term_sem.at[0])

    @pl.when(middle)
    def _():
        for k in range(2):
            left(transit.at[0], transit_send.at[k])

    for zz in range(GROUP):
        left(part_in.at[0], part_sem.at[zz])
        left(rows.at[0, 0], row_send.at[0, zz])
    left(rows.at[0, 0], row_send.at[1, z])

    @pl.when(middle)
    def _():
        for k in range(3):
            left(rows.at[0, 0], row_send.at[2, z + inner * k])


def split_total(total, line):
    top = total.astype(bf16).astype(f32)
    mid = (total - top).astype(bf16).astype(f32)
    low = total - top - mid
    return jnp.where(line == 0, top, jnp.where(line == 1, mid, low)).astype(bf16)


def join_total(parts):
    parts = parts.astype(f32)
    return parts[0:1] + parts[1:2] + parts[2:3]


def fused_local(
    stream,
    queries,
    keys_in,
    values_in,
    gate_in,
    log_decay,
    head_gain,
    out_weight,
    norm_gain,
    gate_weight,
    up_weight,
    down_weight,
):
    count, heads = log_decay.shape
    width = queries.shape[1]
    dim = width // heads
    depth = stream.shape[1]
    own, units = gate_weight.shape
    sizes = GROUP * GROUP
    part = units // GROUP
    down = down_weight.reshape(GROUP, part, down_weight.shape[1])
    half = count // 2
    vmem = pltpu.VMEM
    dma = pltpu.SemaphoreType.DMA
    given = (
        stream,
        queries,
        keys_in,
        values_in,
        gate_in,
        log_decay.T,
        head_gain,
        out_weight,
        norm_gain,
        gate_weight,
        up_weight,
    )
    return pl.pallas_call(
        layer_kernel,
        out_shape=jax.ShapeDtypeStruct((half, depth), bf16),
        in_specs=[pl.BlockSpec(memory_space=pl.ANY)] * 12,
        out_specs=pl.BlockSpec(memory_space=pl.ANY),
        scratch_shapes=[
            *(vmem(value.shape, value.dtype) for value in given),
            vmem((GROUP, own, 2 * part), bf16),
            vmem((sizes, own, 2 * part), bf16),
            vmem((sizes, part, down_weight.shape[1]), bf16),
            vmem((2, part, down_weight.shape[1]), bf16),
            vmem((GROUP, 2, half, depth), bf16),
            vmem((half, depth), f32),
            vmem((heads, count, dim), f32),
            vmem((count, width), f32),
            vmem((heads, dim + TAIL, dim), bf16),
            vmem((heads, dim + TAIL, dim), bf16),
            vmem((dim + TAIL, dim), bf16),
            vmem((GROUP, dim + TAIL, dim), bf16),
            vmem((dim, dim), f32),
            vmem((1, dim), f32),
            vmem((heads, dim, dim), bf16),
            vmem((heads, dim, dim), bf16),
            vmem((count, width), bf16),
            vmem((half, depth), bf16),
            vmem((half, depth), bf16),
            vmem((GROUP, count, part), bf16),
            vmem((GROUP, GROUP, 2, half, depth // GROUP), bf16),
            vmem((GROUP, GROUP, half, depth // GROUP), bf16),
            vmem((GROUP, GROUP, half, depth // GROUP), f32),
            vmem((GROUP, GROUP, half, depth // GROUP), bf16),
            vmem((2, GROUP, GROUP, half, depth // GROUP), bf16),
            vmem((half, depth), bf16),
            dma((12,)),
            dma((GROUP,)),
            dma((2, 2)),
            dma((2, 2)),
            dma((2, sizes, 2)),
            dma((2, GROUP - 1)),
            dma((2,)),
            dma((2,)),
            dma((3,)),
            dma((3,)),
            dma((3,)),
            dma((GROUP,)),
            dma((3,)),
            dma((3,)),
            dma((2,)),
            dma((3, GROUP)),
            dma((2, GROUP, PIECES)),
            dma((GROUP,)),
            dma((GROUP, GROUP)),
            dma((GROUP,)),
            dma((2, GROUP, GROUP)),
        ],
        compiler_params=pltpu.CompilerParams(
            collective_id=0, has_side_effects=True, vmem_limit_bytes=60 * 1024 * 1024
        ),
        name="layer",
    )(*given, down)


def fused(mesh):
    return jax.shard_map(
        fused_local,
        mesh=mesh,
        in_specs=(
            P(("sp", "tp"), None),
            P("sp", "tp"),
            P("sp", "tp"),
            P("sp", "tp"),
            P("sp", "tp"),
            P("sp", "tp"),
            P("tp"),
            P("tp", None),
            P(),
            P("sp", "tp"),
            P("sp", "tp"),
            P("tp", "sp"),
        ),
        out_specs=P(("sp", "tp"), None),
        check_vma=False,
    )


def solution(mesh):
    if fits(mesh):
        return fused(mesh)
    devices = mesh.devices
    count, pair = devices.shape
    split = Mesh(devices.reshape(GROUP, count // GROUP, pair), (*SP, "tp"))
    return jax.shard_map(
        local,
        mesh=split,
        in_specs=(
            P((*SP, "tp"), None),
            P(SP, "tp"),
            P(SP, "tp"),
            P(SP, "tp"),
            P(SP, "tp"),
            P(SP, "tp"),
            P("tp"),
            P("tp", None),
            P(),
            P(SP, "tp"),
            P(SP, "tp"),
            P("tp", SP),
        ),
        out_specs=P((*SP, "tp"), None),
        check_vma=False,
    )
```
